256 devices in a mesh: ep: 64 (over z, x, core), tp: 4 (over y).
Axes of the slice: x: 4, y: 4, z: 8, core: 2. Of those that a mesh axis runs over, the one named last changes fastest.
Arguments:
- residual: bfloat16 [2048, 2048], P('ep'), may hold values from -6 to 6
- routes: int32 [2048, 4], P('ep'), may hold values from 0 to 63, as said below
- lengths: int32 [2048], P('ep'), may hold values from 1 to 512, as said below
- key_cache: bfloat16 [2048, 512, 4, 128], P('ep', None, 'tp'), may hold values from -6 to 6
- value_cache: bfloat16 [2048, 512, 4, 128], P('ep', None, 'tp'), may hold values from -6 to 6
- mix_gain: float32 [2048], replicated, may hold values from 0.1 to 1.9
- w_query: bfloat16 [2048, 2048], P(None, 'tp'), may hold values from -0.125 to 0.125
- w_out: bfloat16 [2048, 2048], P('tp'), may hold values from -0.375 to 0.375
- head_bias: float32 [16], P('tp'), may hold values from -7 to -1
- moe_gain: float32 [2048], replicated, may hold values from 0.1 to 1.9
- w_group: bfloat16 [2048, 8], replicated, may hold values from -0.02734375 to 0.02734375
- w_expert: bfloat16 [2048, 64], replicated, may hold values from -0.02734375 to 0.02734375
- expert_gate: bfloat16 [64, 2048, 1024], P('ep', None, 'tp'), may hold values from -0.125 to 0.125
- expert_up: bfloat16 [64, 2048, 1024], P('ep', None, 'tp'), may hold values from -0.125 to 0.125
- expert_down: bfloat16 [64, 1024, 2048], P('ep', 'tp'), may hold values from -3 to 3
Outputs:
- layer_out: bfloat16 [2048, 2048], P('ep', 'tp')
The draws below stay inside these ranges and needn't reach their ends.
Inputs may be any that keep to these rules, and one draw needn't show every extreme that they name: `routes`: each row names 4 different experts, all in one group of 8 consecutive experts. Within the rows of one device (aligned blocks of 32 rows) no expert is named more than 4 times, and some expert is named exactly 4 times in every block. `lengths`: some sequence has 512 cached positions in every draw.
All inputs are finite; a program needn't handle non-finite values.
Results may differ from the reference program's by a relative error of at most 0.02.
Values may be sent and summed in bfloat16 or wider, within the bound.
No kernel may reach another device: no remote copies, remote signals or barrier semaphores. Data moves between devices by JAX's collectives and lax.ppermute only.
A program may use at most 64 MiB of HBM per device.

```python
import jax
import jax.numpy as jnp
from jax import lax

D = 2048
HEADS = 16
HEAD_SIZE = 128
KV_HEADS = 4
FF = 1024
GROUP_SIZE = 8
TOPK = 4
SEQ_DEV = 32
CACHE = 512
SEQS = 2048
EXPERTS = 64
GROUPS = 8
GROUP_MOST = 8
CAPACITY = 4
N_TP = 4


def draw_routes(key, part):
    streams = jax.random.split(jax.random.fold_in(key, 11), 4)
    blocks = SEQS // SEQ_DEV
    groups = EXPERTS // GROUP_SIZE
    warmth = jax.random.randint(streams[0], (1, groups), 0, 4)
    jitter = jax.random.randint(streams[1], (blocks, groups), 0, 4)
    ranking = (warmth + jitter) * groups + jnp.arange(groups, dtype=jnp.int32)[None, :]
    ordering = jnp.argsort(-ranking, axis=1)
    shuffle = jax.random.randint(streams[2], (blocks, SEQ_DEV), 0, SEQ_DEV) * SEQ_DEV + jnp.arange(SEQ_DEV, dtype=jnp.int32)[None, :]
    ranked = jnp.argsort(jnp.argsort(shuffle, axis=1), axis=1)
    group_id = jnp.take_along_axis(ordering, ranked // GROUP_MOST, axis=1)
    within = ranked % GROUP_MOST
    rotate = jax.random.randint(streams[3], (blocks, groups), 0, GROUP_SIZE)
    offset = jnp.take_along_axis(rotate, group_id, axis=1)
    member = (offset[:, :, None] + within[:, :, None] * TOPK + jnp.arange(TOPK, dtype=jnp.int32)[None, None, :]) % GROUP_SIZE
    return (group_id[:, :, None] * GROUP_SIZE + member).reshape(SEQS, TOPK).astype(jnp.int32)


def draw_lengths(key, part):
    streams = jax.random.split(jax.random.fold_in(key, 23), 3)
    blocks = SEQS // SEQ_DEV
    levels = jax.random.randint(streams[0], (blocks, 1), 1, 9)
    drawn = jax.random.randint(streams[1], (blocks, SEQ_DEV), 1, CACHE + 1)
    scaled = (1 + (drawn - 1) * levels // 8).reshape(SEQS)
    chosen = jax.random.randint(streams[2], (), 0, SEQS)
    filled = jnp.where(jnp.arange(SEQS, dtype=jnp.int32) == chosen, CACHE, scaled)
    return filled.astype(jnp.int32)


def shard_levels(key, extent, cuts, least, high):
    gain, own = 1.0, jax.random.fold_in(key, 6)
    for position, blocks in cuts:
        steps = jnp.exp(jax.random.uniform(jax.random.fold_in(own, position), (blocks,), jnp.float32, least / len(cuts), high / len(cuts)))
        gain = gain * jnp.repeat(steps, extent[position] // blocks).reshape([-1 if axis == position else 1 for axis in range(len(extent))])
    return gain


def noise(stream_key, dims, deviation, bound, shards=(), kind=jnp.bfloat16):
    level = shard_levels(stream_key, dims, shards, -0.22, 0.18) if shards else 1.0
    array = jax.random.normal(stream_key, dims, jnp.float32) * deviation * level
    return jnp.minimum(jnp.maximum(array, -bound), bound).astype(kind)


def setup_inputs(seed: int = 0) -> dict:
    seeds = jax.random.split(jax.random.key(seed), 16)
    return {
        "residual": noise(seeds[0], (SEQS, D), 1.0, 6.0, ((0, 64),)),
        "routes": draw_routes(jax.random.fold_in(seeds[15], 71), 0),
        "lengths": draw_lengths(jax.random.fold_in(seeds[15], 71), 0),
        "key_cache": noise(seeds[3], (SEQS, CACHE, KV_HEADS, HEAD_SIZE), 1.0, 6.0, ((0, 64), (2, 4))),
        "value_cache": noise(seeds[4], (SEQS, CACHE, KV_HEADS, HEAD_SIZE), 1.0, 6.0, ((0, 64), (2, 4))),
        "mix_gain": jnp.clip(1.0 + 0.18 * jax.random.normal(seeds[5], (D,), jnp.float32), 0.1, 1.9),
        "w_query": noise(seeds[6], (D, HEADS * HEAD_SIZE), D ** -0.5, 0.125, ((1, 4),)),
        "w_out": noise(seeds[7], (HEADS * HEAD_SIZE, D), (HEADS * HEAD_SIZE // 9) ** -0.5, 0.375, ((0, 4),)),
        "head_bias": jnp.clip(-7.0 + 6.0 * jax.random.uniform(seeds[8], (HEADS,), jnp.float32) ** shard_levels(seeds[8], (HEADS,), ((0, 4),), -0.2, 0.2), -7.0, -1.0),
        "moe_gain": jnp.clip(1.0 + 0.18 * jax.random.normal(seeds[9], (D,), jnp.float32), 0.1, 1.9),
        "w_group": noise(seeds[10], (D, GROUPS), (25 * D) ** -0.5, 0.02734375),
        "w_expert": noise(seeds[11], (D, EXPERTS), (25 * D) ** -0.5, 0.02734375),
        "expert_gate": noise(seeds[12], (EXPERTS, D, FF), D ** -0.5, 0.125, ((0, 64), (2, 4))),
        "expert_up": noise(seeds[13], (EXPERTS, D, FF), D ** -0.5, 0.125, ((0, 64), (2, 4))),
        "expert_down": noise(seeds[14], (EXPERTS, FF, D), (max(1, FF // 256)) ** -0.5, 3.0, ((0, 64), (1, 4))),
    }


EPSILON = 1e-06

def rms_scale(tokens, gains):
    values = tokens.astype(jnp.float32)
    inverse = lax.rsqrt(lax.optimization_barrier(jnp.mean(values * values, axis=-1, keepdims=True)) + EPSILON)
    return (values * inverse * gains.astype(jnp.float32)).astype(jnp.bfloat16)

def rounded(values):
    return lax.optimization_barrier(values.astype(jnp.bfloat16)).astype(jnp.float32)

def place_rows(buffer, target, source):
    return buffer.at[target].set(source)

def reference(residual, routes, lengths, key_cache, value_cache, mix_gain, w_query, w_out, head_bias, moe_gain, w_group, w_expert, expert_gate, expert_up, expert_down):
    tokens = residual.shape[0]
    normed = rms_scale(residual, mix_gain)
    queries = jnp.dot(normed, w_query, preferred_element_type=jnp.float32).astype(jnp.bfloat16)
    key_heads = key_cache.shape[2]
    head_size = key_cache.shape[3]
    per_key = HEADS // key_heads
    bias_grid = head_bias.astype(jnp.float32).reshape(key_heads, per_key)
    grouped = queries.reshape(tokens, key_heads, per_key, head_size)

    def stick_one(item):
        query_rows, key_rows, value_rows, length = item
        scores = jnp.einsum('kgd,lkd->kgl', query_rows.astype(jnp.float32), key_rows.astype(jnp.float32)) * head_size ** (-0.5)
        scores = scores + bias_grid[:, :, None]
        inside = lax.broadcasted_iota(jnp.int32, scores.shape, 2) < length
        remain = jnp.where(inside, jax.nn.log_sigmoid(-scores), 0.0)
        later_sum = lax.cumsum(remain, axis=2, reverse=True) - remain
        weights = jnp.where(inside, jnp.exp(jax.nn.log_sigmoid(scores) + later_sum), 0.0)
        mixture = jnp.einsum('kgl,lkd->kgd', rounded(weights), value_rows.astype(jnp.float32))
        return mixture.astype(jnp.bfloat16)
    attended = lax.map(stick_one, (grouped, key_cache, value_cache, lengths)).reshape(tokens, HEADS * head_size)
    block = HEADS * head_size // N_TP
    head_part = jnp.einsum('tpc,pcd->ptd', attended.reshape(tokens, N_TP, block).astype(jnp.float32), w_out.reshape(N_TP, block, D).astype(jnp.float32))
    attn_out = lax.optimization_barrier(jnp.sum(rounded(head_part), axis=0)).astype(jnp.bfloat16)
    mid = (residual.astype(jnp.float32) + attn_out.astype(jnp.float32)).astype(jnp.bfloat16)
    hidden_in = rms_scale(mid, moe_gain)
    group_prob = jax.nn.softmax(jnp.dot(hidden_in, w_group, preferred_element_type=jnp.float32), axis=-1)
    expert_logit = jnp.dot(hidden_in, w_expert, preferred_element_type=jnp.float32)
    picked = jnp.take_along_axis(expert_logit, routes, axis=1)
    top_prob = jnp.take_along_axis(group_prob, routes[:, :1] // GROUP_SIZE, axis=1)
    share = jax.nn.softmax(picked, axis=1) * top_prob
    expert_count = w_expert.shape[1]
    blocks = tokens // SEQ_DEV
    block_routes = routes.reshape(blocks, SEQ_DEV * TOPK)
    onehot = (block_routes[:, :, None] == jnp.arange(expert_count, dtype=jnp.int32)[None, None, :]).astype(jnp.int32)
    earlier = jnp.cumsum(onehot, axis=1, dtype=jnp.int32) - onehot
    slot = lax.optimization_barrier(jnp.sum(earlier * onehot, axis=2, dtype=jnp.int32)).astype(jnp.int32)
    target = (block_routes * CAPACITY + slot).astype(jnp.int32)
    source_rows = jnp.repeat(hidden_in.reshape(blocks, SEQ_DEV, D), TOPK, axis=1)
    buffer = jnp.zeros((blocks, expert_count * CAPACITY, D), jnp.bfloat16)
    buffer = jax.vmap(place_rows)(buffer, target, source_rows)
    arranged = buffer.reshape(blocks, expert_count, CAPACITY, D).transpose(1, 0, 2, 3).reshape(expert_count, blocks * CAPACITY, D)
    slab = FF // N_TP

    def run_expert(item):
        batch_rows, gate_weight, up_weight, down_weight = item
        gate = jnp.dot(batch_rows, gate_weight, preferred_element_type=jnp.float32)
        upward = jnp.dot(batch_rows, up_weight, preferred_element_type=jnp.float32)
        active = (jax.nn.silu(gate) * upward).astype(jnp.bfloat16)
        parts = jnp.einsum('rpf,pfd->prd', active.reshape(-1, N_TP, slab).astype(jnp.float32), down_weight.reshape(N_TP, slab, D).astype(jnp.float32))
        return lax.optimization_barrier(jnp.sum(rounded(parts), axis=0)).astype(jnp.bfloat16)
    outputs = lax.map(run_expert, (arranged, expert_gate, expert_up, expert_down))
    outputs = outputs.reshape(expert_count, blocks, CAPACITY, D)
    block_index = jnp.arange(tokens * TOPK, dtype=jnp.int32) // (SEQ_DEV * TOPK)
    pair_out = outputs[routes.reshape(-1), block_index, slot.reshape(-1)].reshape(tokens, TOPK, D)
    moe = lax.optimization_barrier(jnp.sum(share[:, :, None] * pair_out.astype(jnp.float32), axis=1))
    return (mid.astype(jnp.float32) + moe).astype(jnp.bfloat16)
```

```python
import jax
import jax.numpy as jnp
from jax import lax
from jax.sharding import PartitionSpec as P

GROUP_SIZE = 8
TOPK = 4
NZ = 8
NX = 4
NC = 2
EXTRA = 128


EPSILON = 1e-06


def rms_scale(tokens, gains):
    values = tokens.astype(jnp.float32)
    inverse = lax.rsqrt(jnp.mean(values * values, axis=-1, keepdims=True) + EPSILON)
    return (values * inverse * gains).astype(jnp.bfloat16)


def ep_index(z, x, c):
    return (z % NZ) * (NX * NC) + (x % NX) * NC + c % NC


def x_shift(value, step):
    perm = [
        (ep_index(z, x, c), ep_index(z, x + step, c))
        for z in range(NZ)
        for x in range(NX)
        for c in range(NC)
    ]
    return lax.ppermute(value, "ep", perm)


def core_swap(value):
    perm = [(i, i ^ 1) for i in range(NZ * NX * NC)]
    return lax.ppermute(value, "ep", perm)


def tp_shift(value, step):
    n = lax.axis_size("tp")
    return lax.ppermute(value, "tp", [(i, (i + step) % n) for i in range(n)])


def z_exchange(value):
    groups = [[z * NX * NC + r for z in range(NZ)] for r in range(NX * NC)]
    return lax.all_to_all(
        value, "ep", split_axis=0, concat_axis=0, axis_index_groups=groups, tiled=True
    )


def split_bf16(value, parts):
    out = []
    for _ in range(parts):
        part = lax.reduce_precision(value, 8, 7).astype(jnp.bfloat16)
        out.append(part)
        value = value - part.astype(jnp.float32)
    return out


def stick_read(queries, key_rows, value_rows, head_bias, lengths):
    seq_count = queries.shape[0]
    head_size = key_rows.shape[3]
    heads = head_bias.shape[0]
    cache = key_rows.shape[1]
    grouped = queries.reshape(seq_count, heads, head_size)
    keys = key_rows.reshape(seq_count, cache, head_size)
    values = value_rows.reshape(seq_count, cache, head_size)
    scores = jnp.einsum("tgd,tld->tgl", grouped, keys, preferred_element_type=jnp.float32)
    scores = scores * head_size ** (-0.5) + head_bias.reshape(1, heads, 1)
    inside = lax.broadcasted_iota(jnp.int32, scores.shape, 2) < lengths[:, None, None]
    remain = jnp.where(inside, jax.nn.log_sigmoid(-scores), 0.0)
    pos = jnp.arange(cache, dtype=jnp.int32)
    later = (pos[:, None] >= pos[None, :]).astype(jnp.bfloat16)
    flat = remain.reshape(seq_count * heads, cache)
    total = sum(
        jnp.dot(part, later, preferred_element_type=jnp.float32) for part in split_bf16(flat, 3)
    ).reshape(scores.shape)
    weights = jnp.where(inside, jnp.exp(scores + total), 0.0).astype(jnp.bfloat16)
    mixture = jnp.einsum("tgl,tld->tgd", weights, values, preferred_element_type=jnp.float32)
    return mixture.astype(jnp.bfloat16).reshape(seq_count, heads * head_size)


def f32(value):
    return value.astype(jnp.float32)


def per_device(
    residual,
    routes,
    lengths,
    key_cache,
    value_cache,
    mix_gain,
    w_query,
    w_out,
    head_bias,
    moe_gain,
    w_group,
    w_expert,
    expert_gate,
    expert_up,
    expert_down,
):
    bf16 = jnp.bfloat16
    seq_count, width = residual.shape
    n_tp = lax.axis_size("tp")
    tp = lax.axis_index("tp")
    me = lax.axis_index("ep")
    core = me % NC
    own_width = width // n_tp
    expert_count = w_expert.shape[1]
    group_count = w_group.shape[1]

    normed = rms_scale(residual, mix_gain)
    queries = jnp.dot(normed, w_query, preferred_element_type=jnp.float32).astype(bf16)
    attended = stick_read(queries, key_cache, value_cache, head_bias, lengths)
    head_part = jnp.dot(attended, w_out, preferred_element_type=jnp.float32).astype(bf16)
    head_sum = f32(head_part)
    for part in [tp_shift(head_part, step) for step in range(1, n_tp)]:
        head_sum = head_sum + f32(part)
    mid = (f32(residual) + f32(head_sum.astype(bf16))).astype(bf16)
    mid_own = lax.dynamic_slice_in_dim(mid, tp * own_width, own_width, 1)
    hidden_in = rms_scale(mid, moe_gain)

    group_prob = jax.nn.softmax(
        jnp.dot(hidden_in, w_group, preferred_element_type=jnp.float32), axis=-1
    )
    expert_logit = jnp.dot(hidden_in, w_expert, preferred_element_type=jnp.float32)
    expert_ids = jnp.arange(expert_count, dtype=jnp.int32)
    chosen = routes[:, :, None] == expert_ids[None, None, :]
    picked = jnp.sum(jnp.where(chosen, expert_logit[:, None, :], 0.0), axis=2)
    group = routes[:, :1] // GROUP_SIZE
    group_hot = group == jnp.arange(group_count, dtype=jnp.int32)[None, :]
    top_prob = jnp.sum(jnp.where(group_hot, group_prob, 0.0), axis=1, keepdims=True)
    share = jax.nn.softmax(picked, axis=1) * top_prob
    member = routes % GROUP_SIZE
    lanes = jnp.arange(EXTRA // 2, dtype=jnp.int32)
    spread = jnp.sum(
        jnp.where(member[:, :, None] == lanes[None, None, :], share[:, :, None], 0.0), axis=1
    )
    high, low = split_bf16(spread, 2)

    group_row = group[:, 0]
    order = jnp.arange(seq_count, dtype=jnp.int32)
    same = (group_row[:, None] == group_row[None, :]) & (order[None, :] < order[:, None])
    slot = group_row * GROUP_SIZE + jnp.sum(same.astype(jnp.int32), axis=1)
    slots = group_count * GROUP_SIZE
    placing = (jnp.arange(slots, dtype=jnp.int32)[:, None] == slot[None, :]).astype(bf16)
    extended = jnp.concatenate([hidden_in, high, low], axis=1)
    outgoing = jnp.dot(placing, extended, preferred_element_type=jnp.float32).astype(bf16)
    arrived = z_exchange(outgoing.reshape(NZ, GROUP_SIZE, width + EXTRA))
    arrived = arrived.reshape(slots, width + EXTRA)

    own_rows = jnp.stack([arrived] + [x_shift(arrived, step) for step in range(1, NX)])
    other_rows = core_swap(own_rows)
    rows = jnp.concatenate([own_rows, other_rows], axis=0).reshape(NC * NX * slots, width + EXTRA)
    hidden = rows[:, :width]
    extra = f32(rows[:, width:])
    lane = jnp.arange(EXTRA, dtype=jnp.int32) % (EXTRA // 2)
    weight = jnp.sum(
        jnp.where(lane[None, :] == me % GROUP_SIZE, extra, 0.0), axis=1, keepdims=True
    )
    gate = jnp.dot(hidden, expert_gate[0], preferred_element_type=jnp.float32)
    upward = jnp.dot(hidden, expert_up[0], preferred_element_type=jnp.float32)
    active = (jax.nn.silu(gate) * upward).astype(bf16)
    partial = jnp.dot(active, expert_down[0], preferred_element_type=jnp.float32)
    partial = (partial * weight).astype(bf16).reshape(NC, NX * slots, width)
    summed = (f32(partial[0]) + f32(core_swap(partial[1]))).astype(bf16)

    def own_block(value, step):
        start = ((tp + step) % n_tp) * own_width
        return lax.dynamic_slice_in_dim(value, start, own_width, 1)

    total = f32(own_block(summed, 0))
    for part in [tp_shift(own_block(summed, step), step) for step in range(1, n_tp)]:
        total = total + f32(part)
    total = total.astype(bf16).reshape(NX, slots, own_width)
    back = f32(total[0])
    for part in [x_shift(total[step], -step) for step in range(1, NX)]:
        back = back + f32(part)
    returned = z_exchange(back.astype(bf16).reshape(NZ, GROUP_SIZE, own_width))
    returned = returned.reshape(slots, own_width)
    moe = lax.dot_general(
        placing, returned, (((0,), (0,)), ((), ())), preferred_element_type=jnp.float32
    )
    return (f32(mid_own) + moe).astype(bf16)


def solution(mesh):
    in_specs = (
        P("ep", None),
        P("ep", None),
        P("ep"),
        P("ep", None, "tp", None),
        P("ep", None, "tp", None),
        P(),
        P(None, "tp"),
        P("tp", None),
        P("tp"),
        P(),
        P(),
        P(),
        P("ep", None, "tp"),
        P("ep", None, "tp"),
        P("ep", "tp", None),
    )
    out_specs = P("ep", "tp")
    return jax.shard_map(
        per_device, mesh=mesh, in_specs=in_specs, out_specs=out_specs, check_vma=False
    )
```

```python
import jax
import jax.numpy as jnp
from jax import lax
from jax.experimental import pallas as pl
from jax.experimental.pallas import tpu as pltpu
from jax.sharding import PartitionSpec as P

GROUP_SIZE = 8
TOPK = 4
NZ = 8
NX = 4
NC = 2
EXTRA = 128
CHUNK = 128


EPSILON = 1e-06


def rms_scale(tokens, gains):
    values = tokens.astype(jnp.float32)
    inverse = lax.rsqrt(jnp.mean(values * values, axis=-1, keepdims=True) + EPSILON)
    return (values * inverse * gains).astype(jnp.bfloat16)


def ep_index(z, x, c):
    return (z % NZ) * (NX * NC) + (x % NX) * NC + c % NC


def x_shift(value, step):
    perm = [
        (ep_index(z, x, c), ep_index(z, x + step, c))
        for z in range(NZ)
        for x in range(NX)
        for c in range(NC)
    ]
    return lax.ppermute(value, "ep", perm)


def core_swap(value):
    perm = [(i, i ^ 1) for i in range(NZ * NX * NC)]
    return lax.ppermute(value, "ep", perm)


def tp_shift(value, step):
    n = lax.axis_size("tp")
    return lax.ppermute(value, "tp", [(i, (i + step) % n) for i in range(n)])


def z_exchange(value):
    groups = [[z * NX * NC + r for z in range(NZ)] for r in range(NX * NC)]
    return lax.all_to_all(
        value, "ep", split_axis=0, concat_axis=0, axis_index_groups=groups, tiled=True
    )


def split_bf16(value, parts):
    out = []
    for _ in range(parts):
        part = lax.reduce_precision(value, 8, 7).astype(jnp.bfloat16)
        out.append(part)
        value = value - part.astype(jnp.float32)
    return out


def split_in_kernel(value, parts):
    out = []
    for _ in range(parts):
        part = value.astype(jnp.bfloat16)
        out.append(part)
        value = value - part.astype(jnp.float32)
    return out


def attn_kernel(lengths, bias, residual, gain, wq_hbm, k_hbm, v_hbm, wo_hbm, out,
                wq, k, v, wo, q_rows, s_rows, o_rows, wq_sem, wo_sem, k_sem, v_sem):
    seqs, width = residual.shape
    cache = k.shape[1]
    heads = q_rows.shape[0] // seqs
    size = k.shape[2]
    chunks = cache // CHUNK
    rows = seqs * heads
    wq_copy = pltpu.make_async_copy(wq_hbm, wq, wq_sem)
    wo_copy = pltpu.make_async_copy(wo_hbm, wo, wo_sem)
    wq_copy.start()

    def copy(src, dst, sem, t, j):
        part = pl.ds(j * CHUNK, CHUNK)
        return pltpu.make_async_copy(src.at[t, part], dst.at[t, part], sem.at[t, j])

    @pl.loop(0, seqs)
    def _(t):
        for j in range(chunks):
            @pl.when(lengths[t] > j * CHUNK)
            def _():
                copy(k_hbm, k, k_sem, t, j).start()

    @pl.loop(0, seqs)
    def _(t):
        for j in range(chunks):
            @pl.when(lengths[t] > j * CHUNK)
            def _():
                copy(v_hbm, v, v_sem, t, j).start()

            @pl.when(lengths[t] <= j * CHUNK)
            def _():
                v[t, pl.ds(j * CHUNK, CHUNK)] = jnp.zeros((CHUNK, size), v.dtype)

    wo_copy.start()
    x = residual[...].astype(jnp.float32)
    inverse = lax.rsqrt(jnp.mean(x * x, axis=-1, keepdims=True) + EPSILON)
    normed = (x * inverse * gain[...]).astype(jnp.bfloat16)
    r = lax.broadcasted_iota(jnp.int32, (rows, rows), 0)
    c = lax.broadcasted_iota(jnp.int32, (rows, rows), 1)
    perm = (c == (r % heads) * seqs + r // heads).astype(jnp.bfloat16)
    wq_copy.wait()
    q = jnp.dot(normed, wq[...], preferred_element_type=jnp.float32).astype(jnp.bfloat16)
    q_head = jnp.concatenate([q[:, g * size:(g + 1) * size] for g in range(heads)], axis=0)
    q_rows[...] = jnp.dot(perm, q_head, preferred_element_type=jnp.float32)

    per = 8 // heads
    low = lax.broadcasted_iota(jnp.int32, (8, cache), 0) // heads
    low_o = lax.broadcasted_iota(jnp.int32, (8, size), 0) // heads

    @pl.loop(0, seqs // per)
    def _(i):
        at = pl.multiple_of(i * 8, 8)
        q8 = q_rows[pl.ds(at, 8), :].astype(jnp.bfloat16)
        total = None
        for u in range(per):
            t = i * per + u
            for j in range(chunks):
                @pl.when(lengths[t] > j * CHUNK)
                def _():
                    copy(k_hbm, k, k_sem, t, j).wait()
            s = lax.dot_general(q8, k[t], (((1,), (1,)), ((), ())), preferred_element_type=jnp.float32)
            inside = lax.broadcasted_iota(jnp.int32, (8, cache), 1) < lengths[t]
            s = jnp.where(inside, s, -jnp.inf)
            total = s if total is None else jnp.where(low == u, s, total)
        s_rows[pl.ds(at, 8), :] = total

    raw = s_rows[...]
    inside = raw > -jnp.inf
    g = lax.broadcasted_iota(jnp.int32, (rows, 1), 0) % heads
    b = jnp.zeros((rows, 1), jnp.float32)
    for n in range(heads):
        b = jnp.where(g == n, bias[n], b)
    z = jnp.where(inside, raw, 0.0) * size ** (-0.5) + b
    remain = jnp.where(inside, -(jnp.maximum(z, 0.0) + jnp.log1p(jnp.exp(-jnp.abs(z)))), 0.0)
    a = lax.broadcasted_iota(jnp.int32, (cache, cache), 0)
    d = lax.broadcasted_iota(jnp.int32, (cache, cache), 1)
    later = (a >= d).astype(jnp.bfloat16)
    total = sum(jnp.dot(p, later, preferred_element_type=jnp.float32) for p in split_in_kernel(remain, 3))
    s_rows[...] = jnp.where(inside, jnp.exp(z + total), 0.0)

    @pl.loop(0, seqs // per)
    def _(i):
        at = pl.multiple_of(i * 8, 8)
        w8 = s_rows[pl.ds(at, 8), :].astype(jnp.bfloat16)
        total = None
        for u in range(per):
            t = i * per + u
            for j in range(chunks):
                @pl.when(lengths[t] > j * CHUNK)
                def _():
                    copy(v_hbm, v, v_sem, t, j).wait()
            o = jnp.dot(w8, v[t], preferred_element_type=jnp.float32)
            total = o if total is None else jnp.where(low_o == u, o, total)
        o_rows[pl.ds(at, 8), :] = total

    o_head = lax.dot_general(perm, o_rows[...].astype(jnp.bfloat16), (((0,), (0,)), ((), ())),
                             preferred_element_type=jnp.float32).astype(jnp.bfloat16)
    att = jnp.concatenate([o_head[n * seqs:(n + 1) * seqs] for n in range(heads)], axis=1)
    wo_copy.wait()
    out[...] = jnp.dot(att, wo[...], preferred_element_type=jnp.float32).astype(out.dtype)


def attention(residual, gain, w_query, w_out, bias, lengths, keys, values):
    seqs, width = residual.shape
    heads = bias.shape[0]
    cache, size = keys.shape[1:]
    hbm = pl.BlockSpec(memory_space=pltpu.HBM)
    vmem = pl.BlockSpec(memory_space=pltpu.VMEM)
    smem = pl.BlockSpec(memory_space=pltpu.SMEM)
    chunks = cache // CHUNK
    return pl.pallas_call(
        attn_kernel,
        out_shape=pltpu.VMEM((seqs, w_out.shape[1]), jnp.bfloat16),
        in_specs=[smem, smem, vmem, vmem, hbm, hbm, hbm, hbm],
        out_specs=vmem,
        scratch_shapes=[
            pltpu.VMEM(w_query.shape, jnp.bfloat16),
            pltpu.VMEM(keys.shape, jnp.bfloat16),
            pltpu.VMEM(values.shape, jnp.bfloat16),
            pltpu.VMEM(w_out.shape, jnp.bfloat16),
            pltpu.VMEM((seqs * heads, size), jnp.float32),
            pltpu.VMEM((seqs * heads, cache), jnp.float32),
            pltpu.VMEM((seqs * heads, size), jnp.float32),
            pltpu.SemaphoreType.DMA(()),
            pltpu.SemaphoreType.DMA(()),
            pltpu.SemaphoreType.DMA((seqs, chunks)),
            pltpu.SemaphoreType.DMA((seqs, chunks)),
        ],
        name="attend",
    )(lengths, bias, residual, gain.reshape(1, width), w_query, keys, values, w_out)


def f32(value):
    return value.astype(jnp.float32)


def per_device(
    residual,
    routes,
    lengths,
    key_cache,
    value_cache,
    mix_gain,
    w_query,
    w_out,
    head_bias,
    moe_gain,
    w_group,
    w_expert,
    expert_gate,
    expert_up,
    expert_down,
):
    bf16 = jnp.bfloat16
    seq_count, width = residual.shape
    n_tp = lax.axis_size("tp")
    tp = lax.axis_index("tp")
    me = lax.axis_index("ep")
    core = me % NC
    own_width = width // n_tp
    expert_count = w_expert.shape[1]
    group_count = w_group.shape[1]

    head_part = attention(
        residual,
        mix_gain,
        w_query,
        w_out,
        head_bias,
        lengths,
        key_cache.reshape(key_cache.shape[0], key_cache.shape[1], key_cache.shape[3]),
        value_cache.reshape(value_cache.shape[0], value_cache.shape[1], value_cache.shape[3]),
    )
    head_sum = f32(head_part)
    for part in [tp_shift(head_part, step) for step in range(1, n_tp)]:
        head_sum = head_sum + f32(part)
    mid = (f32(residual) + f32(head_sum.astype(bf16))).astype(bf16)
    mid_own = lax.dynamic_slice_in_dim(mid, tp * own_width, own_width, 1)
    hidden_in = rms_scale(mid, moe_gain)

    group_prob = jax.nn.softmax(
        jnp.dot(hidden_in, w_group, preferred_element_type=jnp.float32), axis=-1
    )
    expert_logit = jnp.dot(hidden_in, w_expert, preferred_element_type=jnp.float32)
    expert_ids = jnp.arange(expert_count, dtype=jnp.int32)
    chosen = routes[:, :, None] == expert_ids[None, None, :]
    picked = jnp.sum(jnp.where(chosen, expert_logit[:, None, :], 0.0), axis=2)
    group = routes[:, :1] // GROUP_SIZE
    group_hot = group == jnp.arange(group_count, dtype=jnp.int32)[None, :]
    top_prob = jnp.sum(jnp.where(group_hot, group_prob, 0.0), axis=1, keepdims=True)
    share = jax.nn.softmax(picked, axis=1) * top_prob
    member = routes % GROUP_SIZE
    lanes = jnp.arange(EXTRA // 2, dtype=jnp.int32)
    spread = jnp.sum(
        jnp.where(member[:, :, None] == lanes[None, None, :], share[:, :, None], 0.0), axis=1
    )
    high, low = split_bf16(spread, 2)

    group_row = group[:, 0]
    order = jnp.arange(seq_count, dtype=jnp.int32)
    same = (group_row[:, None] == group_row[None, :]) & (order[None, :] < order[:, None])
    slot = group_row * GROUP_SIZE + jnp.sum(same.astype(jnp.int32), axis=1)
    slots = group_count * GROUP_SIZE
    placing = (jnp.arange(slots, dtype=jnp.int32)[:, None] == slot[None, :]).astype(bf16)
    extended = jnp.concatenate([hidden_in, high, low], axis=1)
    outgoing = jnp.dot(placing, extended, preferred_element_type=jnp.float32).astype(bf16)
    arrived = z_exchange(outgoing.reshape(NZ, GROUP_SIZE, width + EXTRA))
    arrived = arrived.reshape(slots, width + EXTRA)

    own_rows = jnp.stack([arrived] + [x_shift(arrived, step) for step in range(1, NX)])
    other_rows = core_swap(own_rows)
    rows = jnp.concatenate([own_rows, other_rows], axis=0).reshape(NC * NX * slots, width + EXTRA)
    hidden = rows[:, :width]
    extra = f32(rows[:, width:])
    lane = jnp.arange(EXTRA, dtype=jnp.int32) % (EXTRA // 2)
    weight = jnp.sum(
        jnp.where(lane[None, :] == me % GROUP_SIZE, extra, 0.0), axis=1, keepdims=True
    )
    gate = jnp.dot(hidden, expert_gate[0], preferred_element_type=jnp.float32)
    upward = jnp.dot(hidden, expert_up[0], preferred_element_type=jnp.float32)
    active = (jax.nn.silu(gate) * upward).astype(bf16)
    partial = jnp.dot(active, expert_down[0], preferred_element_type=jnp.float32)
    partial = (partial * weight).astype(bf16).reshape(NC, NX * slots, width)
    summed = (f32(partial[0]) + f32(core_swap(partial[1]))).astype(bf16)

    def own_block(value, step):
        start = ((tp + step) % n_tp) * own_width
        return lax.dynamic_slice_in_dim(value, start, own_width, 1)

    total = f32(own_block(summed, 0))
    for part in [tp_shift(own_block(summed, step), step) for step in range(1, n_tp)]:
        total = total + f32(part)
    total = total.astype(bf16).reshape(NX, slots, own_width)
    back = f32(total[0])
    for part in [x_shift(total[step], -step) for step in range(1, NX)]:
        back = back + f32(part)
    returned = z_exchange(back.astype(bf16).reshape(NZ, GROUP_SIZE, own_width))
    returned = returned.reshape(slots, own_width)
    moe = lax.dot_general(
        placing, returned, (((0,), (0,)), ((), ())), preferred_element_type=jnp.float32
    )
    return (f32(mid_own) + moe).astype(bf16)


def solution(mesh):
    in_specs = (
        P("ep", None),
        P("ep", None),
        P("ep"),
        P("ep", None, "tp", None),
        P("ep", None, "tp", None),
        P(),
        P(None, "tp"),
        P("tp", None),
        P("tp"),
        P(),
        P(),
        P(),
        P("ep", None, "tp"),
        P("ep", None, "tp"),
        P("ep", "tp", None),
    )
    out_specs = P("ep", "tp")
    return jax.shard_map(
        per_device, mesh=mesh, in_specs=in_specs, out_specs=out_specs, check_vma=False
    )
```

```python
import functools

import jax
import jax.numpy as jnp
from jax import lax
from jax.experimental import pallas as pl
from jax.experimental.pallas import tpu as pltpu
from jax.sharding import PartitionSpec as P


GROUP_SIZE = 8
NZ = 8
NX = 4
NC = 2
EXTRA = 128
COPIES = 4


EPSILON = 1e-06


def rms_scale(tokens, gains):
    values = tokens.astype(jnp.float32)
    inverse = lax.rsqrt(jnp.mean(values * values, axis=-1, keepdims=True) + EPSILON)
    return (values * inverse * gains).astype(jnp.bfloat16)


def ep_index(z, x, c):
    return (z % NZ) * (NX * NC) + (x % NX) * NC + c % NC


def x_shift(value, step):
    perm = [
        (ep_index(z, x, c), ep_index(z, x + step, c))
        for z in range(NZ)
        for x in range(NX)
        for c in range(NC)
    ]
    return lax.ppermute(value, "ep", perm)


def core_swap(value):
    perm = [(i, i ^ 1) for i in range(NZ * NX * NC)]
    return lax.ppermute(value, "ep", perm)


def tp_shift(value, step):
    n = lax.axis_size("tp")
    return lax.ppermute(value, "tp", [(i, (i + step) % n) for i in range(n)])


def z_exchange(value):
    groups = [[z * NX * NC + r for z in range(NZ)] for r in range(NX * NC)]
    return lax.all_to_all(
        value, "ep", split_axis=0, concat_axis=0, axis_index_groups=groups, tiled=True
    )


def split_bf16(value, parts):
    out = []
    for _ in range(parts):
        part = lax.reduce_precision(value, 8, 7).astype(jnp.bfloat16)
        out.append(part)
        value = value - part.astype(jnp.float32)
    return out


def split_in_kernel(value, parts):
    out = []
    for _ in range(parts):
        part = value.astype(jnp.bfloat16)
        out.append(part)
        value = value - part.astype(jnp.float32)
    return out


def attn_kernel(lengths, bias, residual, gain, wq_hbm, k_hbm, v_hbm, wo_hbm, out,
                wq, k, v, wo, q_rows, s_rows, o_rows, wq_sem, wo_sem, k_sem, v_sem):
    seqs, _ = residual.shape
    cache = k.shape[1]
    heads = q_rows.shape[0] // seqs
    size = k.shape[2]
    rows = seqs * heads
    groups = k_sem.shape[0]
    each = seqs // groups
    wq_copy = pltpu.make_async_copy(wq_hbm, wq, wq_sem)
    wo_copy = pltpu.make_async_copy(wo_hbm, wo, wo_sem)

    def copy(src, dst, sem, n):
        part = pl.ds(n * each, each)
        return pltpu.make_async_copy(src.at[part], dst.at[part], sem.at[n])

    k_copies = [copy(k_hbm, k, k_sem, n) for n in range(groups)]
    v_copies = [copy(v_hbm, v, v_sem, n) for n in range(groups)]
    for piece in [wq_copy, *k_copies, *v_copies, wo_copy]:
        piece.start()
    x = residual[...].astype(jnp.float32)
    inverse = lax.rsqrt(jnp.mean(x * x, axis=-1, keepdims=True) + EPSILON)
    normed = (x * inverse * gain[...]).astype(jnp.bfloat16)
    r = lax.broadcasted_iota(jnp.int32, (rows, rows), 0)
    c = lax.broadcasted_iota(jnp.int32, (rows, rows), 1)
    perm = (c == (r % heads) * seqs + r // heads).astype(jnp.bfloat16)
    row = lax.broadcasted_iota(jnp.int32, (rows, 1), 0)
    b = jnp.zeros((rows, 1), jnp.float32)
    for n in range(heads):
        b = jnp.where(row % heads == n, bias[n], b)
    length = jnp.zeros((rows, 1), jnp.int32)
    for t in range(seqs):
        length = jnp.where(row // heads == t, lengths[t], length)
    inside = lax.broadcasted_iota(jnp.int32, (rows, cache), 1) < length
    wq_copy.wait()
    q = jnp.dot(normed, wq[...], preferred_element_type=jnp.float32).astype(jnp.bfloat16)
    q_head = jnp.concatenate([q[:, g * size:(g + 1) * size] for g in range(heads)], axis=0)
    q_rows[...] = jnp.dot(perm, q_head, preferred_element_type=jnp.float32)

    per = 8 // heads
    low = lax.broadcasted_iota(jnp.int32, (8, cache), 0) // heads
    low_o = lax.broadcasted_iota(jnp.int32, (8, size), 0) // heads
    for n in range(groups):
        k_copies[n].wait()
        for i in range(n * each // per, (n + 1) * each // per):
            q8 = q_rows[i * 8:(i + 1) * 8, :].astype(jnp.bfloat16)
            total = None
            for u in range(per):
                s = lax.dot_general(q8, k[i * per + u], (((1,), (1,)), ((), ())),
                                    preferred_element_type=jnp.float32)
                total = s if total is None else jnp.where(low == u, s, total)
            s_rows[i * 8:(i + 1) * 8, :] = total

    z = s_rows[...] * size ** (-0.5) + b
    remain = jnp.where(inside, -(jnp.maximum(z, 0.0) + jnp.log1p(jnp.exp(-jnp.abs(z)))), 0.0)
    first = lax.broadcasted_iota(jnp.int32, (cache, cache), 0)
    second = lax.broadcasted_iota(jnp.int32, (cache, cache), 1)
    later = (first >= second).astype(jnp.bfloat16)
    total = sum(
        jnp.dot(p, later, preferred_element_type=jnp.float32) for p in split_in_kernel(remain, 3)
    )
    s_rows[...] = jnp.where(inside, jnp.exp(z + total), 0.0)

    for n in range(groups):
        v_copies[n].wait()
        for i in range(n * each // per, (n + 1) * each // per):
            w8 = s_rows[i * 8:(i + 1) * 8, :].astype(jnp.bfloat16)
            total = None
            for u in range(per):
                o = jnp.dot(w8, v[i * per + u], preferred_element_type=jnp.float32)
                total = o if total is None else jnp.where(low_o == u, o, total)
            o_rows[i * 8:(i + 1) * 8, :] = total

    o_head = lax.dot_general(perm, o_rows[...].astype(jnp.bfloat16), (((0,), (0,)), ((), ())),
                             preferred_element_type=jnp.float32).astype(jnp.bfloat16)
    att = jnp.concatenate([o_head[n * seqs:(n + 1) * seqs] for n in range(heads)], axis=1)
    wo_copy.wait()
    out[...] = jnp.dot(att, wo[...], preferred_element_type=jnp.float32).astype(out.dtype)


def attention(residual, gain, w_query, w_out, bias, lengths, keys, values):
    seqs, width = residual.shape
    heads = bias.shape[0]
    cache, size = keys.shape[1:]
    hbm = pl.BlockSpec(memory_space=pltpu.HBM)
    vmem = pl.BlockSpec(memory_space=pltpu.VMEM)
    smem = pl.BlockSpec(memory_space=pltpu.SMEM)
    return pl.pallas_call(
        attn_kernel,
        out_shape=pltpu.VMEM((seqs, w_out.shape[1]), jnp.bfloat16),
        in_specs=[smem, smem, vmem, vmem, hbm, hbm, hbm, hbm],
        out_specs=vmem,
        scratch_shapes=[
            pltpu.VMEM(w_query.shape, jnp.bfloat16),
            pltpu.VMEM(keys.shape, jnp.bfloat16),
            pltpu.VMEM(values.shape, jnp.bfloat16),
            pltpu.VMEM(w_out.shape, jnp.bfloat16),
            pltpu.VMEM((seqs * heads, size), jnp.float32),
            pltpu.VMEM((seqs * heads, cache), jnp.float32),
            pltpu.VMEM((seqs * heads, size), jnp.float32),
            pltpu.SemaphoreType.DMA(()),
            pltpu.SemaphoreType.DMA(()),
            pltpu.SemaphoreType.DMA((COPIES,)),
            pltpu.SemaphoreType.DMA((COPIES,)),
        ],
        name="attend",
    )(lengths, bias, residual, gain.reshape(1, width), w_query, keys, values, w_out)


def expert_kernel(count, steps, place, *refs):
    pieces = refs[:count]
    gate_w, up_w, down_w = refs[count : count + 3]
    blocks = refs[count + 3 : count + 3 + steps]
    sent = refs[count + 3 + steps]
    width = gate_w.shape[0]
    rows = jnp.concatenate([piece[:, :width] for piece in pieces], axis=0)
    extra = jnp.concatenate([piece[:, width:] for piece in pieces], axis=0).astype(jnp.float32)
    lane = lax.broadcasted_iota(jnp.int32, extra.shape, 1) % (EXTRA // 2)
    weight = jnp.sum(jnp.where(lane == place[1], extra, 0.0), axis=1, keepdims=True)
    gate = jnp.dot(rows, gate_w[...], preferred_element_type=jnp.float32)
    upward = jnp.dot(rows, up_w[...], preferred_element_type=jnp.float32)
    active = (gate / (1.0 + jnp.exp(-gate)) * upward).astype(jnp.bfloat16)
    own = blocks[0].shape[0]
    block = blocks[0].shape[1]
    for step in range(steps):
        start = pl.multiple_of(lax.rem(place[0] + step, steps) * block, block)
        down = down_w[:, pl.ds(start, block)]
        part = jnp.dot(active, down, preferred_element_type=jnp.float32) * weight
        part = part.astype(jnp.bfloat16)
        blocks[step][...] = part[:own]
        sent[step] = part[own:]


def experts(place, ours, theirs, weights, steps):
    width = weights[2].shape[1]
    rows = sum(piece.shape[0] for piece in ours)
    block = width // steps
    vmem = pl.BlockSpec(memory_space=pltpu.VMEM)
    out = pl.pallas_call(
        functools.partial(expert_kernel, len(ours) + len(theirs), steps),
        out_shape=[pltpu.VMEM((rows, block), jnp.bfloat16)] * steps
        + [pltpu.VMEM((steps, rows, block), jnp.bfloat16)],
        in_specs=[pl.BlockSpec(memory_space=pltpu.SMEM)]
        + [vmem] * (len(ours) + len(theirs) + 3),
        out_specs=[vmem] * (steps + 1),
        compiler_params=pltpu.CompilerParams(vmem_limit_bytes=16 << 20),
        cost_estimate=pl.CostEstimate(
            flops=2 * 2 * rows * 3 * width * weights[0].shape[1],
            transcendentals=2 * rows * weights[0].shape[1],
            bytes_accessed=0,
        ),
        name="experts",
    )(place, *ours, *theirs, *weights)
    return out[:steps], out[steps]


def add_kernel(steps, *refs):
    blocks, arrived, outs = refs[:steps], refs[steps], refs[steps + 1 :]
    for step in range(steps):
        total = blocks[step][...].astype(jnp.float32) + arrived[step].astype(jnp.float32)
        outs[step][...] = total.astype(jnp.bfloat16)


def add_blocks(blocks, arrived):
    steps = len(blocks)
    vmem = pl.BlockSpec(memory_space=pltpu.VMEM)
    return pl.pallas_call(
        functools.partial(add_kernel, steps),
        out_shape=[pltpu.VMEM(blocks[0].shape, jnp.bfloat16)] * steps,
        in_specs=[vmem] * (steps + 1),
        out_specs=[vmem] * steps,
        compiler_params=pltpu.CompilerParams(vmem_limit_bytes=4 << 20),
        name="add_blocks",
    )(*blocks, arrived)


def f32(value):
    return value.astype(jnp.float32)


def per_device(
    residual,
    routes,
    lengths,
    key_cache,
    value_cache,
    mix_gain,
    w_query,
    w_out,
    head_bias,
    moe_gain,
    w_group,
    w_expert,
    expert_gate,
    expert_up,
    expert_down,
):
    bf16 = jnp.bfloat16
    seq_count, width = residual.shape
    n_tp = lax.axis_size("tp")
    tp = lax.axis_index("tp")
    me = lax.axis_index("ep")
    own_width = width // n_tp
    expert_count = w_expert.shape[1]
    group_count = w_group.shape[1]

    head_part = attention(
        residual,
        mix_gain,
        w_query,
        w_out,
        head_bias,
        lengths,
        key_cache.reshape(key_cache.shape[0], key_cache.shape[1], key_cache.shape[3]),
        value_cache.reshape(value_cache.shape[0], value_cache.shape[1], value_cache.shape[3]),
    )
    head_sum = f32(head_part)
    for part in [tp_shift(head_part, step) for step in range(1, n_tp)]:
        head_sum = head_sum + f32(part)
    mid = (f32(residual) + f32(head_sum.astype(bf16))).astype(bf16)
    mid_own = lax.dynamic_slice_in_dim(mid, tp * own_width, own_width, 1)
    hidden_in = rms_scale(mid, moe_gain)

    group_prob = jax.nn.softmax(
        jnp.dot(hidden_in, w_group, preferred_element_type=jnp.float32), axis=-1
    )
    expert_logit = jnp.dot(hidden_in, w_expert, preferred_element_type=jnp.float32)
    expert_ids = jnp.arange(expert_count, dtype=jnp.int32)
    chosen = routes[:, :, None] == expert_ids[None, None, :]
    picked = jnp.sum(jnp.where(chosen, expert_logit[:, None, :], 0.0), axis=2)
    group = routes[:, :1] // GROUP_SIZE
    group_hot = group == jnp.arange(group_count, dtype=jnp.int32)[None, :]
    top_prob = jnp.sum(jnp.where(group_hot, group_prob, 0.0), axis=1, keepdims=True)
    share = jax.nn.softmax(picked, axis=1) * top_prob
    member = routes % GROUP_SIZE
    lanes = jnp.arange(EXTRA // 2, dtype=jnp.int32)
    spread = jnp.sum(
        jnp.where(member[:, :, None] == lanes[None, None, :], share[:, :, None], 0.0), axis=1
    )
    high, low = split_bf16(spread, 2)

    group_row = group[:, 0]
    order = jnp.arange(seq_count, dtype=jnp.int32)
    same = (group_row[:, None] == group_row[None, :]) & (order[None, :] < order[:, None])
    slot = group_row * GROUP_SIZE + jnp.sum(same.astype(jnp.int32), axis=1)
    slots = group_count * GROUP_SIZE
    placing = (jnp.arange(slots, dtype=jnp.int32)[:, None] == slot[None, :]).astype(bf16)
    extended = jnp.concatenate([hidden_in, high, low], axis=1)
    outgoing = jnp.dot(placing, extended, preferred_element_type=jnp.float32).astype(bf16)
    arrived = z_exchange(outgoing.reshape(NZ, GROUP_SIZE, width + EXTRA))
    arrived = arrived.reshape(slots, width + EXTRA)

    half = slots // 2
    place = jnp.stack([tp, me % GROUP_SIZE]).astype(jnp.int32)
    weights = (expert_gate[0], expert_up[0], expert_down[0])

    def chunk(pieces):
        theirs = []
        for piece in pieces:
            theirs.append(core_swap(piece))
        blocks, sent = experts(place, pieces, theirs, weights, n_tp)
        sent = core_swap(sent)
        blocks = add_blocks(blocks, sent)
        total = f32(blocks[0])
        for step in range(1, n_tp):
            part = tp_shift(blocks[step], step)
            total = total + f32(part)
        return total.astype(bf16)

    left = x_shift(arrived, 1)
    right = x_shift(arrived, -1)
    near = chunk([arrived])
    relay0 = x_shift(left[:half], 1)
    relay1 = x_shift(right[half:], -1)
    sides = chunk([left, right])
    far = chunk([relay0, relay1])
    back0 = x_shift(sides[:slots], -1)
    back1 = x_shift(sides[slots:], 1)
    back2 = x_shift(far, 2)
    back = f32(near) + f32(back0) + f32(back1) + f32(back2)
    returned = z_exchange(back.astype(bf16).reshape(NZ, GROUP_SIZE, own_width))
    returned = returned.reshape(slots, own_width)
    moe = lax.dot_general(
        placing, returned, (((0,), (0,)), ((), ())), preferred_element_type=jnp.float32
    )
    return (f32(mid_own) + moe).astype(bf16)


def solution(mesh):
    in_specs = (
        P("ep", None),
        P("ep", None),
        P("ep"),
        P("ep", None, "tp", None),
        P("ep", None, "tp", None),
        P(),
        P(None, "tp"),
        P("tp", None),
        P("tp"),
        P(),
        P(),
        P(),
        P("ep", None, "tp"),
        P("ep", None, "tp"),
        P("ep", "tp", None),
    )
    out_specs = P("ep", "tp")
    return jax.shard_map(
        per_device, mesh=mesh, in_specs=in_specs, out_specs=out_specs, check_vma=False
    )
```

```python
import functools

import jax
import jax.numpy as jnp
from jax import lax
from jax.experimental import pallas as pl
from jax.experimental.pallas import tpu as pltpu
from jax.sharding import PartitionSpec as P


GROUP_SIZE = 8
TOPK = 4
NZ = 8
NX = 4
NC = 2
EXTRA = 128
COPIES = 4


EPSILON = 1e-06


def ep_index(z, x, c):
    return (z % NZ) * (NX * NC) + (x % NX) * NC + c % NC


def x_shift(value, step):
    perm = [
        (ep_index(z, x, c), ep_index(z, x + step, c))
        for z in range(NZ)
        for x in range(NX)
        for c in range(NC)
    ]
    return lax.ppermute(value, "ep", perm)


def core_swap(value):
    perm = [(i, i ^ 1) for i in range(NZ * NX * NC)]
    return lax.ppermute(value, "ep", perm)


def tp_shift(value, step):
    n = lax.axis_size("tp")
    return lax.ppermute(value, "tp", [(i, (i + step) % n) for i in range(n)])


def z_exchange(value):
    groups = [[z * NX * NC + r for z in range(NZ)] for r in range(NX * NC)]
    return lax.all_to_all(
        value, "ep", split_axis=0, concat_axis=0, axis_index_groups=groups, tiled=True
    )


def split_in_kernel(value, parts):
    out = []
    for _ in range(parts):
        part = value.astype(jnp.bfloat16)
        out.append(part)
        value = value - part.astype(jnp.float32)
    return out


def attn_kernel(lengths, bias, residual, gain, wq_hbm, k_hbm, v_hbm, wo_hbm, out,
                wq, k, v, wo, q_rows, s_rows, o_rows, wq_sem, wo_sem, k_sem, v_sem):
    seqs, _ = residual.shape
    cache = k.shape[1]
    heads = q_rows.shape[0] // seqs
    size = k.shape[2]
    rows = seqs * heads
    groups = k_sem.shape[0]
    each = seqs // groups
    wq_copy = pltpu.make_async_copy(wq_hbm, wq, wq_sem)
    wo_copy = pltpu.make_async_copy(wo_hbm, wo, wo_sem)

    def copy(src, dst, sem, n):
        part = pl.ds(n * each, each)
        return pltpu.make_async_copy(src.at[part], dst.at[part], sem.at[n])

    k_copies = [copy(k_hbm, k, k_sem, n) for n in range(groups)]
    v_copies = [copy(v_hbm, v, v_sem, n) for n in range(groups)]
    for piece in [wq_copy, *k_copies, *v_copies, wo_copy]:
        piece.start()
    x = residual[...].astype(jnp.float32)
    inverse = lax.rsqrt(jnp.mean(x * x, axis=-1, keepdims=True) + EPSILON)
    normed = (x * inverse * gain[...]).astype(jnp.bfloat16)
    r = lax.broadcasted_iota(jnp.int32, (rows, rows), 0)
    c = lax.broadcasted_iota(jnp.int32, (rows, rows), 1)
    perm = (c == (r % heads) * seqs + r // heads).astype(jnp.bfloat16)
    row = lax.broadcasted_iota(jnp.int32, (rows, 1), 0)
    b = jnp.zeros((rows, 1), jnp.float32)
    for n in range(heads):
        b = jnp.where(row % heads == n, bias[n], b)
    length = jnp.zeros((rows, 1), jnp.int32)
    for t in range(seqs):
        length = jnp.where(row // heads == t, lengths[t], length)
    inside = lax.broadcasted_iota(jnp.int32, (rows, cache), 1) < length
    wq_copy.wait()
    q = jnp.dot(normed, wq[...], preferred_element_type=jnp.float32).astype(jnp.bfloat16)
    q_head = jnp.concatenate([q[:, g * size:(g + 1) * size] for g in range(heads)], axis=0)
    q_rows[...] = jnp.dot(perm, q_head, preferred_element_type=jnp.float32)

    per = 8 // heads
    low = lax.broadcasted_iota(jnp.int32, (8, cache), 0) // heads
    low_o = lax.broadcasted_iota(jnp.int32, (8, size), 0) // heads
    for n in range(groups):
        k_copies[n].wait()
        for i in range(n * each // per, (n + 1) * each // per):
            q8 = q_rows[i * 8:(i + 1) * 8, :].astype(jnp.bfloat16)
            total = None
            for u in range(per):
                s = lax.dot_general(q8, k[i * per + u], (((1,), (1,)), ((), ())),
                                    preferred_element_type=jnp.float32)
                total = s if total is None else jnp.where(low == u, s, total)
            s_rows[i * 8:(i + 1) * 8, :] = total

    z = s_rows[...] * size ** (-0.5) + b
    remain = jnp.where(inside, -(jnp.maximum(z, 0.0) + jnp.log1p(jnp.exp(-jnp.abs(z)))), 0.0)
    first = lax.broadcasted_iota(jnp.int32, (cache, cache), 0)
    second = lax.broadcasted_iota(jnp.int32, (cache, cache), 1)
    later = (first >= second).astype(jnp.bfloat16)
    total = sum(
        jnp.dot(p, later, preferred_element_type=jnp.float32) for p in split_in_kernel(remain, 3)
    )
    s_rows[...] = jnp.where(inside, jnp.exp(z + total), 0.0)

    for n in range(groups):
        v_copies[n].wait()
        for i in range(n * each // per, (n + 1) * each // per):
            w8 = s_rows[i * 8:(i + 1) * 8, :].astype(jnp.bfloat16)
            total = None
            for u in range(per):
                o = jnp.dot(w8, v[i * per + u], preferred_element_type=jnp.float32)
                total = o if total is None else jnp.where(low_o == u, o, total)
            o_rows[i * 8:(i + 1) * 8, :] = total

    o_head = lax.dot_general(perm, o_rows[...].astype(jnp.bfloat16), (((0,), (0,)), ((), ())),
                             preferred_element_type=jnp.float32).astype(jnp.bfloat16)
    att = jnp.concatenate([o_head[n * seqs:(n + 1) * seqs] for n in range(heads)], axis=1)
    wo_copy.wait()
    out[...] = jnp.dot(att, wo[...], preferred_element_type=jnp.float32).astype(out.dtype)


def attention(residual, gain, w_query, w_out, bias, lengths, keys, values):
    seqs, width = residual.shape
    heads = bias.shape[0]
    cache, size = keys.shape[1:]
    hbm = pl.BlockSpec(memory_space=pltpu.HBM)
    vmem = pl.BlockSpec(memory_space=pltpu.VMEM)
    smem = pl.BlockSpec(memory_space=pltpu.SMEM)
    return pl.pallas_call(
        attn_kernel,
        out_shape=pltpu.VMEM((seqs, w_out.shape[1]), jnp.bfloat16),
        in_specs=[smem, smem, vmem, vmem, hbm, hbm, hbm, hbm],
        out_specs=vmem,
        scratch_shapes=[
            pltpu.VMEM(w_query.shape, jnp.bfloat16),
            pltpu.VMEM(keys.shape, jnp.bfloat16),
            pltpu.VMEM(values.shape, jnp.bfloat16),
            pltpu.VMEM(w_out.shape, jnp.bfloat16),
            pltpu.VMEM((seqs * heads, size), jnp.float32),
            pltpu.VMEM((seqs * heads, cache), jnp.float32),
            pltpu.VMEM((seqs * heads, size), jnp.float32),
            pltpu.SemaphoreType.DMA(()),
            pltpu.SemaphoreType.DMA(()),
            pltpu.SemaphoreType.DMA((COPIES,)),
            pltpu.SemaphoreType.DMA((COPIES,)),
        ],
        name="attend",
    )(lengths, bias, residual, gain.reshape(1, width), w_query, keys, values, w_out)


def call(kernel, outs, args, flops=0, vmem=16):
    in_vmem = pl.BlockSpec(memory_space=pltpu.VMEM)
    in_smem = pl.BlockSpec(memory_space=pltpu.SMEM)
    return pl.pallas_call(
        kernel,
        out_shape=[pltpu.VMEM(shape, dtype) for shape, dtype in outs],
        in_specs=[in_smem if arg.ndim == 1 else in_vmem for arg in args],
        out_specs=[in_vmem] * len(outs),
        compiler_params=pltpu.CompilerParams(vmem_limit_bytes=vmem << 20),
        cost_estimate=pl.CostEstimate(flops=flops, transcendentals=0, bytes_accessed=0),
    )(*args)


def route_kernel(count, place, *refs):
    parts = refs[:count]
    residual, gain, group_w, expert_w, routes, outgoing, mid_own, placing = refs[count:]
    total = sum(part[...].astype(jnp.float32) for part in parts)
    mid = residual[...].astype(jnp.float32) + total.astype(jnp.bfloat16).astype(jnp.float32)
    mid = mid.astype(jnp.bfloat16)
    values = mid.astype(jnp.float32)
    seqs, width = values.shape
    inverse = lax.rsqrt(jnp.mean(values * values, axis=-1, keepdims=True) + EPSILON)
    hidden = (values * inverse * gain[...]).astype(jnp.bfloat16)

    def logits(weight):
        return lax.dot_general(
            hidden, weight[...], (((1,), (1,)), ((), ())), preferred_element_type=jnp.float32
        )

    group_logit = logits(group_w)
    expert_logit = logits(expert_w)
    named = [routes[:, k : k + 1] for k in range(TOPK)]
    group = jnp.right_shift(named[0], 3)
    member = [jnp.bitwise_and(one, GROUP_SIZE - 1) for one in named]
    lane_e = lax.broadcasted_iota(jnp.int32, expert_logit.shape, 1)
    lane_g = lax.broadcasted_iota(jnp.int32, group_logit.shape, 1)
    picked = [
        jnp.sum(jnp.where(lane_e == one, expert_logit, 0.0), axis=1, keepdims=True)
        for one in named
    ]
    most = functools.reduce(jnp.maximum, picked)
    powers = [jnp.exp(one - most) for one in picked]
    group_power = jnp.exp(group_logit - jnp.max(group_logit, axis=1, keepdims=True))
    in_group = lane_g == group
    top = jnp.sum(jnp.where(in_group, group_power, 0.0), axis=1, keepdims=True)
    top = top / jnp.sum(group_power, axis=1, keepdims=True)
    scale = top / sum(powers)
    lane = lax.broadcasted_iota(jnp.int32, (seqs, EXTRA), 1)
    half = EXTRA // 2
    spread = jnp.zeros((seqs, EXTRA), jnp.float32)
    for one, power in zip(member, powers):
        spread = jnp.where(jnp.bitwise_and(lane, half - 1) == one, power * scale, spread)
    high = spread.astype(jnp.bfloat16).astype(jnp.float32)
    extra = jnp.where(lane < half, high, spread - high).astype(jnp.bfloat16)
    before = lax.broadcasted_iota(jnp.int32, (seqs, seqs), 0)
    before = before > lax.broadcasted_iota(jnp.int32, (seqs, seqs), 1)
    hot = in_group.astype(jnp.float32)
    earlier = jnp.dot(
        before.astype(jnp.bfloat16), hot.astype(jnp.bfloat16), preferred_element_type=jnp.float32
    )
    rank = jnp.sum(earlier * hot, axis=1, keepdims=True).astype(jnp.int32)
    slot = group * GROUP_SIZE + rank
    slots = outgoing.shape[0]
    puts = (lax.broadcasted_iota(jnp.int32, (seqs, slots), 1) == slot).astype(jnp.bfloat16)
    placing[...] = puts

    def placed(value):
        out = lax.dot_general(
            puts, value, (((0,), (0,)), ((), ())), preferred_element_type=jnp.float32
        )
        return out.astype(jnp.bfloat16)

    outgoing[:, :width] = placed(hidden)
    outgoing[:, width:] = placed(extra)
    own = mid_own.shape[1]
    low = lax.broadcasted_iota(jnp.int32, (1, 1), 0) + place[0]
    kept = jnp.zeros(mid_own.shape, jnp.float32)
    for n in range(width // own):
        kept = jnp.where(low == n, values[:, n * own : (n + 1) * own], kept)
    mid_own[...] = kept.astype(jnp.bfloat16)


def expert_kernel(count, place, *refs):
    pieces = refs[:count]
    gate_w, up_w, down_w, kept, sent = refs[count:]
    width = gate_w.shape[0]
    rows = jnp.concatenate([piece[:, :width] for piece in pieces], axis=0)
    extra = jnp.concatenate([piece[:, width:] for piece in pieces], axis=0).astype(jnp.float32)
    lane = lax.broadcasted_iota(jnp.int32, extra.shape, 1)
    mine = jnp.bitwise_and(lane, EXTRA // 2 - 1) == place[1]
    weight = jnp.sum(jnp.where(mine, extra, 0.0), axis=1, keepdims=True)
    gate = jnp.dot(rows, gate_w[...], preferred_element_type=jnp.float32)
    upward = jnp.dot(rows, up_w[...], preferred_element_type=jnp.float32)
    active = (gate / (1.0 + jnp.exp(-gate)) * upward).astype(jnp.bfloat16)
    part = jnp.dot(active, down_w[...], preferred_element_type=jnp.float32) * weight
    own = kept.shape[0]
    kept[...] = part[:own].astype(jnp.bfloat16)
    sent[...] = part[own:].astype(jnp.bfloat16)


def experts(place, ours, theirs, weights):
    width = weights[2].shape[1]
    rows = sum(piece.shape[0] for piece in ours)
    out = ((rows, width), jnp.bfloat16)
    count = len(ours) + len(theirs)
    flops = 2 * 2 * rows * 3 * width * weights[0].shape[1]
    kernel = functools.partial(expert_kernel, count)
    return call(kernel, [out, out], [place, *ours, *theirs, *weights], flops)


def add_kernel(kept, arrived, *outs):
    rows = outs[0].shape[0]
    for n, out in enumerate(outs):
        part = slice(n * rows, (n + 1) * rows)
        total = kept[part].astype(jnp.float32) + arrived[part].astype(jnp.float32)
        out[...] = total.astype(jnp.bfloat16)


def block_kernel(count, place, *refs):
    parts, outs = refs[:count], refs[count:]
    steps, block = len(outs), outs[0].shape[1]
    for step in range(steps):
        start = pl.multiple_of(lax.rem(place[0] + step, steps) * block, block)
        part = pl.ds(start, block)
        total = sum(one[:, part].astype(jnp.float32) for one in parts)
        outs[step][...] = total.astype(jnp.bfloat16)


def sum_kernel(*refs):
    refs[-1][...] = sum(one[...].astype(jnp.float32) for one in refs[:-1]).astype(jnp.bfloat16)


def last_kernel(mid_own, placing, returned, out):
    moe = jnp.dot(placing[...], returned[...], preferred_element_type=jnp.float32)
    out[...] = (mid_own[...].astype(jnp.float32) + moe).astype(jnp.bfloat16)


def per_device(
    residual,
    routes,
    lengths,
    key_cache,
    value_cache,
    mix_gain,
    w_query,
    w_out,
    head_bias,
    moe_gain,
    w_group,
    w_expert,
    expert_gate,
    expert_up,
    expert_down,
):
    bf16 = jnp.bfloat16
    seq_count, width = residual.shape
    n_tp = lax.axis_size("tp")
    tp = lax.axis_index("tp")
    me = lax.axis_index("ep")
    own_width = width // n_tp
    slots = w_group.shape[1] * GROUP_SIZE
    place = jnp.stack([tp, me % GROUP_SIZE]).astype(jnp.int32)
    weights = (expert_gate[0], expert_up[0], expert_down[0])

    head_part = attention(
        residual,
        mix_gain,
        w_query,
        w_out,
        head_bias,
        lengths,
        key_cache.reshape(key_cache.shape[0], key_cache.shape[1], key_cache.shape[3]),
        value_cache.reshape(value_cache.shape[0], value_cache.shape[1], value_cache.shape[3]),
    )
    head_parts = [head_part]
    for step in (1, 3, 2):
        head_parts.append(tp_shift(head_part, step))
    outgoing, mid_own, placing = call(
        functools.partial(route_kernel, n_tp),
        [
            ((slots, width + EXTRA), bf16),
            ((seq_count, own_width), bf16),
            ((seq_count, slots), bf16),
        ],
        [
            place,
            *head_parts,
            residual,
            moe_gain.reshape(1, width),
            w_group.T,
            w_expert.T,
            routes,
        ],
    )
    arrived = z_exchange(outgoing.reshape(NZ, GROUP_SIZE, width + EXTRA))
    arrived = arrived.reshape(slots, width + EXTRA)

    def chunk(pieces):
        theirs = []
        for piece in pieces:
            theirs.append(core_swap(piece))
        kept, sent = experts(place, pieces, theirs, weights)
        return kept, core_swap(sent)

    def added(pair, count):
        rows = pair[0].shape[0] // count
        return call(add_kernel, [((rows, width), bf16)] * count, list(pair), vmem=8)

    half = slots // 2
    left = x_shift(arrived, 1)
    right = x_shift(arrived, -1)
    near = chunk([arrived])
    relay0 = x_shift(left[:half], 1)
    relay1 = x_shift(right[half:], -1)
    to_left, to_right = added(chunk([left, right]), 2)
    back0 = x_shift(to_left, -1)
    back1 = x_shift(to_right, 1)
    (to_far,) = added(chunk([relay0, relay1]), 1)
    back2 = x_shift(to_far, 2)
    parts = [*near, back0, back1, back2]
    blocks = call(
        functools.partial(block_kernel, len(parts)),
        [((slots, own_width), bf16)] * n_tp,
        [place, *parts],
        vmem=8,
    )
    summed = [blocks[0]]
    for step in (1, 3, 2):
        summed.append(tp_shift(blocks[step], step))
    (total,) = call(sum_kernel, [((slots, own_width), bf16)], summed, vmem=4)
    returned = z_exchange(total.reshape(NZ, GROUP_SIZE, own_width)).reshape(slots, own_width)
    vmem = pl.BlockSpec(memory_space=pltpu.VMEM)
    return pl.pallas_call(
        last_kernel,
        out_shape=jax.ShapeDtypeStruct((seq_count, own_width), bf16),
        in_specs=[vmem] * 3,
        out_specs=vmem,
        compiler_params=pltpu.CompilerParams(vmem_limit_bytes=4 << 20),
        name="last",
    )(mid_own, placing, returned)


def solution(mesh):
    in_specs = (
        P("ep", None),
        P("ep", None),
        P("ep"),
        P("ep", None, "tp", None),
        P("ep", None, "tp", None),
        P(),
        P(None, "tp"),
        P("tp", None),
        P("tp"),
        P(),
        P(),
        P(),
        P("ep", None, "tp"),
        P("ep", None, "tp"),
        P("ep", "tp", None),
    )
    out_specs = P("ep", "tp")
    return jax.shard_map(
        per_device, mesh=mesh, in_specs=in_specs, out_specs=out_specs, check_vma=False
    )
```

```python
import functools

import jax
import jax.numpy as jnp
from jax import lax
from jax.experimental import pallas as pl
from jax.experimental.pallas import tpu as pltpu
from jax.sharding import PartitionSpec as P


GROUP_SIZE = 8
TOPK = 4
NZ = 8
NX = 4
NC = 2
EXTRA = 128
COPIES = 4


EPSILON = 1e-06


def ep_index(z, x, c):
    return (z % NZ) * (NX * NC) + (x % NX) * NC + c % NC


def x_shift(value, step):
    perm = [
        (ep_index(z, x, c), ep_index(z, x + step, c))
        for z in range(NZ)
        for x in range(NX)
        for c in range(NC)
    ]
    return lax.ppermute(value, "ep", perm)


def core_swap(value):
    perm = [(i, i ^ 1) for i in range(NZ * NX * NC)]
    return lax.ppermute(value, "ep", perm)


def tp_shift(value, step):
    n = lax.axis_size("tp")
    return lax.ppermute(value, "tp", [(i, (i + step) % n) for i in range(n)])


def z_exchange(value):
    groups = [[z * NX * NC + r for z in range(NZ)] for r in range(NX * NC)]
    return lax.all_to_all(
        value, "ep", split_axis=0, concat_axis=0, axis_index_groups=groups, tiled=True
    )


def split_in_kernel(value, parts):
    out = []
    for _ in range(parts):
        part = value.astype(jnp.bfloat16)
        out.append(part)
        value = value - part.astype(jnp.float32)
    return out


def attn_kernel(lengths, bias, gain_hbm, wq_hbm, k_hbm, v_hbm, wo_hbm, *refs):
    small = refs[:4]
    out, smalls = refs[4], refs[5:9]
    residual = smalls[0]
    (gain, wq, k, v, wo, q_rows, s_rows, o_rows, wq_sem, wo_sem, k_sem, v_sem, small_sem,
     gain_sem) = refs[9:]
    seqs, _ = residual.shape
    cache = k.shape[1]
    heads = q_rows.shape[0] // seqs
    size = k.shape[2]
    rows = seqs * heads
    groups = k_sem.shape[0]
    each = seqs // groups
    wq_copy = pltpu.make_async_copy(wq_hbm, wq, wq_sem)
    wo_copy = pltpu.make_async_copy(wo_hbm, wo, wo_sem)

    def copy(src, dst, sem, n):
        part = pl.ds(n * each, each)
        return pltpu.make_async_copy(src.at[part], dst.at[part], sem.at[n])

    k_copies = [copy(k_hbm, k, k_sem, n) for n in range(groups)]
    v_copies = [copy(v_hbm, v, v_sem, n) for n in range(groups)]
    small_copies = [
        pltpu.make_async_copy(src, dst, small_sem.at[n])
        for n, (src, dst) in enumerate(zip(small, smalls))
    ]
    gain_copy = pltpu.make_async_copy(gain_hbm, gain, gain_sem)
    first = [gain_copy, small_copies[0], wq_copy, *k_copies, *v_copies[:-1]]
    for piece in [*first, wo_copy, v_copies[-1], *small_copies[1:]]:
        piece.start()
    gain_copy.wait()
    small_copies[0].wait()
    x = residual[...].astype(jnp.float32)
    inverse = lax.rsqrt(jnp.mean(x * x, axis=-1, keepdims=True) + EPSILON)
    normed = (x * inverse * gain[...]).astype(jnp.bfloat16)
    r = lax.broadcasted_iota(jnp.int32, (rows, rows), 0)
    c = lax.broadcasted_iota(jnp.int32, (rows, rows), 1)
    perm = (c == (r % heads) * seqs + r // heads).astype(jnp.bfloat16)
    row = lax.broadcasted_iota(jnp.int32, (rows, 1), 0)
    b = jnp.zeros((rows, 1), jnp.float32)
    for n in range(heads):
        b = jnp.where(row % heads == n, bias[n], b)
    length = jnp.zeros((rows, 1), jnp.int32)
    for t in range(seqs):
        length = jnp.where(row // heads == t, lengths[t], length)
    inside = lax.broadcasted_iota(jnp.int32, (rows, cache), 1) < length
    wq_copy.wait()
    q = jnp.dot(normed, wq[...], preferred_element_type=jnp.float32).astype(jnp.bfloat16)
    q_head = jnp.concatenate([q[:, g * size:(g + 1) * size] for g in range(heads)], axis=0)
    q_rows[...] = jnp.dot(perm, q_head, preferred_element_type=jnp.float32)

    per = 8 // heads
    low = lax.broadcasted_iota(jnp.int32, (8, cache), 0) // heads
    low_o = lax.broadcasted_iota(jnp.int32, (8, size), 0) // heads
    for n in range(groups):
        k_copies[n].wait()
        for i in range(n * each // per, (n + 1) * each // per):
            q8 = q_rows[i * 8:(i + 1) * 8, :].astype(jnp.bfloat16)
            total = None
            for u in range(per):
                s = lax.dot_general(q8, k[i * per + u], (((1,), (1,)), ((), ())),
                                    preferred_element_type=jnp.float32)
                total = s if total is None else jnp.where(low == u, s, total)
            s_rows[i * 8:(i + 1) * 8, :] = total

    z = s_rows[...] * size ** (-0.5) + b
    remain = jnp.where(inside, -(jnp.maximum(z, 0.0) + jnp.log1p(jnp.exp(-jnp.abs(z)))), 0.0)
    first = lax.broadcasted_iota(jnp.int32, (cache, cache), 0)
    second = lax.broadcasted_iota(jnp.int32, (cache, cache), 1)
    later = (first >= second).astype(jnp.bfloat16)
    total = sum(
        jnp.dot(p, later, preferred_element_type=jnp.float32) for p in split_in_kernel(remain, 3)
    )
    s_rows[...] = jnp.where(inside, jnp.exp(z + total), 0.0)

    for n in range(groups):
        v_copies[n].wait()
        for i in range(n * each // per, (n + 1) * each // per):
            w8 = s_rows[i * 8:(i + 1) * 8, :].astype(jnp.bfloat16)
            total = None
            for u in range(per):
                o = jnp.dot(w8, v[i * per + u], preferred_element_type=jnp.float32)
                total = o if total is None else jnp.where(low_o == u, o, total)
            o_rows[i * 8:(i + 1) * 8, :] = total

    o_head = lax.dot_general(perm, o_rows[...].astype(jnp.bfloat16), (((0,), (0,)), ((), ())),
                             preferred_element_type=jnp.float32).astype(jnp.bfloat16)
    att = jnp.concatenate([o_head[n * seqs:(n + 1) * seqs] for n in range(heads)], axis=1)
    for piece in small_copies[1:]:
        piece.wait()
    wo_copy.wait()
    out[...] = jnp.dot(att, wo[...], preferred_element_type=jnp.float32).astype(out.dtype)


def attention(residual, gain, w_query, w_out, bias, lengths, keys, values, small):
    seqs, width = residual.shape
    heads = bias.shape[0]
    cache, size = keys.shape[1:]
    hbm = pl.BlockSpec(memory_space=pltpu.HBM)
    vmem = pl.BlockSpec(memory_space=pltpu.VMEM)
    smem = pl.BlockSpec(memory_space=pltpu.SMEM)
    outs = [((seqs, w_out.shape[1]), jnp.bfloat16)] + [(one.shape, one.dtype) for one in small]
    small = [pltpu.with_memory_space_constraint(one, pltpu.HBM) for one in small]
    gain = pltpu.with_memory_space_constraint(gain.reshape(1, width), pltpu.HBM)
    return pl.pallas_call(
        attn_kernel,
        out_shape=[pltpu.VMEM(shape, dtype) for shape, dtype in outs],
        in_specs=[smem, smem] + [hbm] * (5 + len(small)),
        out_specs=[vmem] * len(outs),
        scratch_shapes=[
            pltpu.VMEM((1, width), jnp.float32),
            pltpu.VMEM(w_query.shape, jnp.bfloat16),
            pltpu.VMEM(keys.shape, jnp.bfloat16),
            pltpu.VMEM(values.shape, jnp.bfloat16),
            pltpu.VMEM(w_out.shape, jnp.bfloat16),
            pltpu.VMEM((seqs * heads, size), jnp.float32),
            pltpu.VMEM((seqs * heads, cache), jnp.float32),
            pltpu.VMEM((seqs * heads, size), jnp.float32),
            pltpu.SemaphoreType.DMA(()),
            pltpu.SemaphoreType.DMA(()),
            pltpu.SemaphoreType.DMA((COPIES,)),
            pltpu.SemaphoreType.DMA((COPIES,)),
            pltpu.SemaphoreType.DMA((len(small),)),
            pltpu.SemaphoreType.DMA(()),
        ],
        name="attend",
    )(lengths, bias, gain, w_query, keys, values, w_out, *small)


def call(kernel, outs, args, flops=0, vmem=16):
    in_vmem = pl.BlockSpec(memory_space=pltpu.VMEM)
    in_smem = pl.BlockSpec(memory_space=pltpu.SMEM)
    return pl.pallas_call(
        kernel,
        out_shape=[pltpu.VMEM(shape, dtype) for shape, dtype in outs],
        in_specs=[in_smem if arg.ndim == 1 else in_vmem for arg in args],
        out_specs=[in_vmem] * len(outs),
        compiler_params=pltpu.CompilerParams(vmem_limit_bytes=vmem << 20),
        cost_estimate=pl.CostEstimate(flops=flops, transcendentals=0, bytes_accessed=0),
    )(*args)


def route_kernel(count, *refs):
    parts = refs[:count]
    residual, gain, group_w, expert_w, routes, outgoing, mid_own, placing = refs[count:]
    total = sum(part[...].astype(jnp.float32) for part in parts)
    mid = residual[...].astype(jnp.float32) + total.astype(jnp.bfloat16).astype(jnp.float32)
    mid = mid.astype(jnp.bfloat16)
    values = mid.astype(jnp.float32)
    seqs, width = values.shape
    inverse = lax.rsqrt(jnp.mean(values * values, axis=-1, keepdims=True) + EPSILON)
    hidden = (values * inverse * gain[...]).astype(jnp.bfloat16)

    def logits(weight):
        return lax.dot_general(
            hidden, weight[...], (((1,), (1,)), ((), ())), preferred_element_type=jnp.float32
        )

    group_logit = logits(group_w)
    expert_logit = logits(expert_w)
    eye = lax.broadcasted_iota(jnp.int32, (TOPK, TOPK), 0)
    eye = (eye == lax.broadcasted_iota(jnp.int32, (TOPK, TOPK), 1)).astype(jnp.bfloat16)
    turned = lax.dot_general(
        routes[...].astype(jnp.float32).astype(jnp.bfloat16),
        eye,
        (((0,), (0,)), ((), ())),
        preferred_element_type=jnp.float32,
    ).astype(jnp.int32)
    named = [turned[:, k : k + 1] for k in range(TOPK)]
    group = jnp.right_shift(named[0], 3)
    member = [jnp.bitwise_and(one, GROUP_SIZE - 1) for one in named]
    lane_e = lax.broadcasted_iota(jnp.int32, expert_logit.shape, 1)
    lane_g = lax.broadcasted_iota(jnp.int32, group_logit.shape, 1)
    picked = [
        jnp.sum(jnp.where(lane_e == one, expert_logit, 0.0), axis=1, keepdims=True)
        for one in named
    ]
    most = functools.reduce(jnp.maximum, picked)
    powers = [jnp.exp(one - most) for one in picked]
    group_power = jnp.exp(group_logit - jnp.max(group_logit, axis=1, keepdims=True))
    in_group = lane_g == group
    top = jnp.sum(jnp.where(in_group, group_power, 0.0), axis=1, keepdims=True)
    top = top / jnp.sum(group_power, axis=1, keepdims=True)
    scale = top / sum(powers)
    lane = lax.broadcasted_iota(jnp.int32, (seqs, EXTRA), 1)
    half = EXTRA // 2
    spread = jnp.zeros((seqs, EXTRA), jnp.float32)
    for one, power in zip(member, powers):
        spread = jnp.where(jnp.bitwise_and(lane, half - 1) == one, power * scale, spread)
    high = spread.astype(jnp.bfloat16).astype(jnp.float32)
    extra = jnp.where(lane < half, high, spread - high).astype(jnp.bfloat16)
    before = lax.broadcasted_iota(jnp.int32, (seqs, seqs), 0)
    before = before > lax.broadcasted_iota(jnp.int32, (seqs, seqs), 1)
    hot = in_group.astype(jnp.float32)
    earlier = jnp.dot(
        before.astype(jnp.bfloat16), hot.astype(jnp.bfloat16), preferred_element_type=jnp.float32
    )
    rank = jnp.sum(earlier * hot, axis=1, keepdims=True).astype(jnp.int32)
    slot = group * GROUP_SIZE + rank
    slots = outgoing.shape[0]
    puts = (lax.broadcasted_iota(jnp.int32, (seqs, slots), 1) == slot).astype(jnp.bfloat16)
    placing[...] = puts

    def placed(value):
        out = lax.dot_general(
            puts, value, (((0,), (0,)), ((), ())), preferred_element_type=jnp.float32
        )
        return out.astype(jnp.bfloat16)

    outgoing[:, :width] = placed(hidden)
    outgoing[:, width:] = placed(extra)
    own = mid_own.shape[1]
    low = lax.broadcasted_iota(jnp.int32, (1, 1), 0) + lax.axis_index("tp")
    kept = jnp.zeros(mid_own.shape, jnp.float32)
    for n in range(width // own):
        kept = jnp.where(low == n, values[:, n * own : (n + 1) * own], kept)
    mid_own[...] = kept.astype(jnp.bfloat16)


def fetch_kernel(after, *refs):
    count = (len(refs) - 1) // 2
    sem = refs[-1]
    copies = [
        pltpu.make_async_copy(src, dst, sem.at[n])
        for n, (src, dst) in enumerate(zip(refs[:count], refs[count : 2 * count]))
    ]
    for piece in copies:
        piece.start()
    for piece in copies:
        piece.wait()


def fetched(arrays, after):
    hbm = pl.BlockSpec(memory_space=pltpu.HBM)
    vmem = pl.BlockSpec(memory_space=pltpu.VMEM)
    arrays = [pltpu.with_memory_space_constraint(one, pltpu.HBM) for one in arrays]
    return pl.pallas_call(
        fetch_kernel,
        out_shape=[pltpu.VMEM(one.shape, one.dtype) for one in arrays],
        in_specs=[vmem] + [hbm] * len(arrays),
        out_specs=[vmem] * len(arrays),
        scratch_shapes=[pltpu.SemaphoreType.DMA((len(arrays),))],
        compiler_params=pltpu.CompilerParams(vmem_limit_bytes=4 << 20),
        cost_estimate=pl.CostEstimate(flops=1 << 30, transcendentals=0, bytes_accessed=0),
        name="fetch",
    )(after, *arrays)


def expert_kernel(count, *refs):
    pieces = refs[:count]
    gate_w, up_w, down_w, kept, sent = refs[count:]
    width = gate_w.shape[0]
    rows = jnp.concatenate([piece[:, :width] for piece in pieces], axis=0)
    extra = jnp.concatenate([piece[:, width:] for piece in pieces], axis=0).astype(jnp.float32)
    lane = lax.broadcasted_iota(jnp.int32, extra.shape, 1)
    mine = jnp.bitwise_and(lane, EXTRA // 2 - 1) == lax.rem(lax.axis_index("ep"), GROUP_SIZE)
    weight = jnp.sum(jnp.where(mine, extra, 0.0), axis=1, keepdims=True)
    gate = jnp.dot(rows, gate_w[...], preferred_element_type=jnp.float32)
    upward = jnp.dot(rows, up_w[...], preferred_element_type=jnp.float32)
    active = (gate / (1.0 + jnp.exp(-gate)) * upward).astype(jnp.bfloat16)
    part = jnp.dot(active, down_w[...], preferred_element_type=jnp.float32) * weight
    own = kept.shape[0]
    kept[...] = part[:own].astype(jnp.bfloat16)
    sent[...] = part[own:].astype(jnp.bfloat16)


def experts(ours, theirs, weights):
    width = weights[2].shape[1]
    rows = sum(piece.shape[0] for piece in ours)
    out = ((rows, width), jnp.bfloat16)
    count = len(ours) + len(theirs)
    flops = 2 * 2 * rows * 3 * width * weights[0].shape[1]
    kernel = functools.partial(expert_kernel, count)
    return call(kernel, [out, out], [*ours, *theirs, *weights], flops)


def add_kernel(kept, arrived, *outs):
    rows = outs[0].shape[0]
    for n, out in enumerate(outs):
        part = slice(n * rows, (n + 1) * rows)
        total = kept[part].astype(jnp.float32) + arrived[part].astype(jnp.float32)
        out[...] = total.astype(jnp.bfloat16)


def block_kernel(count, *refs):
    parts, outs = refs[:count], refs[count:]
    steps, block = len(outs), outs[0].shape[1]
    for step in range(steps):
        start = pl.multiple_of(lax.rem(lax.axis_index("tp") + step, steps) * block, block)
        part = pl.ds(start, block)
        total = sum(one[:, part].astype(jnp.float32) for one in parts)
        outs[step][...] = total.astype(jnp.bfloat16)


def sum_kernel(*refs):
    refs[-1][...] = sum(one[...].astype(jnp.float32) for one in refs[:-1]).astype(jnp.bfloat16)


def last_kernel(mid_own, placing, returned, out):
    moe = jnp.dot(placing[...], returned[...], preferred_element_type=jnp.float32)
    out[...] = (mid_own[...].astype(jnp.float32) + moe).astype(jnp.bfloat16)


def per_device(
    residual,
    routes,
    lengths,
    key_cache,
    value_cache,
    mix_gain,
    w_query,
    w_out,
    head_bias,
    moe_gain,
    w_group,
    w_expert,
    expert_gate,
    expert_up,
    expert_down,
):
    bf16 = jnp.bfloat16
    seq_count, width = residual.shape
    n_tp = lax.axis_size("tp")
    own_width = width // n_tp
    slots = w_group.shape[1] * GROUP_SIZE

    head_part, *small = attention(
        residual,
        mix_gain,
        w_query,
        w_out,
        head_bias,
        lengths,
        key_cache.reshape(key_cache.shape[0], key_cache.shape[1], key_cache.shape[3]),
        value_cache.reshape(value_cache.shape[0], value_cache.shape[1], value_cache.shape[3]),
        [residual, moe_gain.reshape(1, width), w_group.T, w_expert.T],
    )
    weights = fetched((expert_gate[0], expert_up[0], expert_down[0]), head_part)
    head_parts = [head_part]
    for step in (1, 3, 2):
        part = tp_shift(head_part, step)
        head_parts.append(pltpu.with_memory_space_constraint(part, pltpu.VMEM))
    outgoing, mid_own, placing = call(
        functools.partial(route_kernel, n_tp),
        [
            ((slots, width + EXTRA), bf16),
            ((seq_count, own_width), bf16),
            ((seq_count, slots), bf16),
        ],
        [
            *head_parts,
            *small,
            routes.T,
        ],
    )
    arrived = z_exchange(outgoing.reshape(NZ, GROUP_SIZE, width + EXTRA))
    arrived = arrived.reshape(slots, width + EXTRA)

    def chunk(pieces):
        theirs = []
        for piece in pieces:
            theirs.append(core_swap(piece))
        kept, sent = experts(pieces, theirs, weights)
        return kept, core_swap(sent)

    def added(pair, count):
        rows = pair[0].shape[0] // count
        return call(add_kernel, [((rows, width), bf16)] * count, list(pair), vmem=8)

    half = slots // 2
    left = x_shift(arrived, 1)
    right = x_shift(arrived, -1)
    near = chunk([arrived])
    relay0 = x_shift(left[:half], 1)
    relay1 = x_shift(right[half:], -1)
    to_left, to_right = added(chunk([left, right]), 2)
    back0 = x_shift(to_left, -1)
    back1 = x_shift(to_right, 1)
    far = chunk([relay0, relay1])

    def y_sum(parts):
        blocks = call(
            functools.partial(block_kernel, len(parts)),
            [((slots, own_width), bf16)] * n_tp,
            list(parts),
            vmem=8,
        )
        summed = [blocks[0]]
        for step in (1, 3, 2):
            summed.append(tp_shift(blocks[step], step))
        return summed

    def total(parts):
        return call(sum_kernel, [((slots, own_width), bf16)], parts, vmem=4)[0]

    to_far = total(y_sum(far))
    own = y_sum([*near, back0, back1])
    back2 = x_shift(to_far, 2)
    total = total([*own, back2])
    returned = z_exchange(total.reshape(NZ, GROUP_SIZE, own_width)).reshape(slots, own_width)
    vmem = pl.BlockSpec(memory_space=pltpu.VMEM)
    return pl.pallas_call(
        last_kernel,
        out_shape=jax.ShapeDtypeStruct((seq_count, own_width), bf16),
        in_specs=[vmem] * 3,
        out_specs=vmem,
        compiler_params=pltpu.CompilerParams(vmem_limit_bytes=4 << 20),
        name="last",
    )(mid_own, placing, returned)


def solution(mesh):
    in_specs = (
        P("ep", None),
        P("ep", None),
        P("ep"),
        P("ep", None, "tp", None),
        P("ep", None, "tp", None),
        P(),
        P(None, "tp"),
        P("tp", None),
        P("tp"),
        P(),
        P(),
        P(),
        P("ep", None, "tp"),
        P("ep", None, "tp"),
        P("ep", "tp", None),
    )
    out_specs = P("ep", "tp")
    return jax.shard_map(
        per_device, mesh=mesh, in_specs=in_specs, out_specs=out_specs, check_vma=False
    )
```

```python
import functools

import jax
import jax.numpy as jnp
from jax import lax
from jax.experimental import pallas as pl
from jax.experimental.pallas import tpu as pltpu
from jax.sharding import PartitionSpec as P


GROUP_SIZE = 8
TOPK = 4
NZ = 8
NX = 4
NC = 2
EXTRA = 128
COPIES = 4


EPSILON = 1e-06


def ep_index(z, x, c):
    return (z % NZ) * (NX * NC) + (x % NX) * NC + c % NC


def x_shift(value, step):
    perm = [
        (ep_index(z, x, c), ep_index(z, x + step, c))
        for z in range(NZ)
        for x in range(NX)
        for c in range(NC)
    ]
    return lax.ppermute(value, "ep", perm)


def core_swap(value):
    perm = [(i, i ^ 1) for i in range(NZ * NX * NC)]
    return lax.ppermute(value, "ep", perm)


def tp_shift(value, step):
    n = lax.axis_size("tp")
    return lax.ppermute(value, "tp", [(i, (i + step) % n) for i in range(n)])


def z_exchange(value):
    groups = [[z * NX * NC + r for z in range(NZ)] for r in range(NX * NC)]
    return lax.all_to_all(
        value, "ep", split_axis=0, concat_axis=0, axis_index_groups=groups, tiled=True
    )


def split_in_kernel(value, parts):
    out = []
    for _ in range(parts):
        part = value.astype(jnp.bfloat16)
        out.append(part)
        value = value - part.astype(jnp.float32)
    return out


def attn_kernel(lengths_hbm, bias_hbm, gain_hbm, wq_hbm, k_hbm, v_hbm, wo_hbm, *refs):
    small = refs[:4]
    out, smalls = refs[4], refs[5:9]
    residual = smalls[0]
    (lengths, bias, gain, wq, k, v, wo, q_rows, s_rows, o_rows, wq_sem, wo_sem, k_sem, v_sem, small_sem,
     gain_sem, lengths_sem, bias_sem) = refs[9:]
    seqs, _ = residual.shape
    cache = k.shape[1]
    heads = q_rows.shape[0] // seqs
    size = k.shape[2]
    rows = seqs * heads
    groups = k_sem.shape[0]
    each = seqs // groups
    wq_copy = pltpu.make_async_copy(wq_hbm, wq, wq_sem)
    wo_copy = pltpu.make_async_copy(wo_hbm, wo, wo_sem)

    def copy(src, dst, sem, n):
        part = pl.ds(n * each, each)
        return pltpu.make_async_copy(src.at[part], dst.at[part], sem.at[n])

    k_copies = [copy(k_hbm, k, k_sem, n) for n in range(groups)]
    v_copies = [copy(v_hbm, v, v_sem, n) for n in range(groups)]
    small_copies = [
        pltpu.make_async_copy(src, dst, small_sem.at[n])
        for n, (src, dst) in enumerate(zip(small, smalls))
    ]
    gain_copy = pltpu.make_async_copy(gain_hbm, gain, gain_sem)
    lengths_copy = pltpu.make_async_copy(lengths_hbm, lengths, lengths_sem)
    bias_copy = pltpu.make_async_copy(bias_hbm, bias, bias_sem)
    lengths_copy.start()
    bias_copy.start()
    first = [gain_copy, small_copies[0], wq_copy, *k_copies, *v_copies[:-1]]
    for piece in [*first, wo_copy, v_copies[-1], *small_copies[1:]]:
        piece.start()
    gain_copy.wait()
    small_copies[0].wait()
    x = residual[...].astype(jnp.float32)
    inverse = lax.rsqrt(jnp.mean(x * x, axis=-1, keepdims=True) + EPSILON)
    normed = (x * inverse * gain[...]).astype(jnp.bfloat16)
    r = lax.broadcasted_iota(jnp.int32, (rows, rows), 0)
    c = lax.broadcasted_iota(jnp.int32, (rows, rows), 1)
    perm = (c == (r % heads) * seqs + r // heads).astype(jnp.bfloat16)
    row = lax.broadcasted_iota(jnp.int32, (rows, 1), 0)
    lengths_copy.wait()
    bias_copy.wait()
    b = jnp.zeros((rows, 1), jnp.float32)
    for n in range(heads):
        b = jnp.where(row % heads == n, bias[n], b)
    length = jnp.zeros((rows, 1), jnp.int32)
    for t in range(seqs):
        length = jnp.where(row // heads == t, lengths[t], length)
    inside = lax.broadcasted_iota(jnp.int32, (rows, cache), 1) < length
    wq_copy.wait()
    q = jnp.dot(normed, wq[...], preferred_element_type=jnp.float32).astype(jnp.bfloat16)
    q_head = jnp.concatenate([q[:, g * size:(g + 1) * size] for g in range(heads)], axis=0)
    q_rows[...] = jnp.dot(perm, q_head, preferred_element_type=jnp.float32)

    per = 8 // heads
    low = lax.broadcasted_iota(jnp.int32, (8, cache), 0) // heads
    low_o = lax.broadcasted_iota(jnp.int32, (8, size), 0) // heads
    for n in range(groups):
        k_copies[n].wait()
        for i in range(n * each // per, (n + 1) * each // per):
            q8 = q_rows[i * 8:(i + 1) * 8, :].astype(jnp.bfloat16)
            total = None
            for u in range(per):
                s = lax.dot_general(q8, k[i * per + u], (((1,), (1,)), ((), ())),
                                    preferred_element_type=jnp.float32)
                total = s if total is None else jnp.where(low == u, s, total)
            s_rows[i * 8:(i + 1) * 8, :] = total

    z = s_rows[...] * size ** (-0.5) + b
    remain = jnp.where(inside, -(jnp.maximum(z, 0.0) + jnp.log1p(jnp.exp(-jnp.abs(z)))), 0.0)
    first = lax.broadcasted_iota(jnp.int32, (cache, cache), 0)
    second = lax.broadcasted_iota(jnp.int32, (cache, cache), 1)
    later = (first >= second).astype(jnp.bfloat16)
    total = sum(
        jnp.dot(p, later, preferred_element_type=jnp.float32) for p in split_in_kernel(remain, 3)
    )
    s_rows[...] = jnp.where(inside, jnp.exp(z + total), 0.0)

    for n in range(groups):
        v_copies[n].wait()
        for i in range(n * each // per, (n + 1) * each // per):
            w8 = s_rows[i * 8:(i + 1) * 8, :].astype(jnp.bfloat16)
            total = None
            for u in range(per):
                o = jnp.dot(w8, v[i * per + u], preferred_element_type=jnp.float32)
                total = o if total is None else jnp.where(low_o == u, o, total)
            o_rows[i * 8:(i + 1) * 8, :] = total

    o_head = lax.dot_general(perm, o_rows[...].astype(jnp.bfloat16), (((0,), (0,)), ((), ())),
                             preferred_element_type=jnp.float32).astype(jnp.bfloat16)
    att = jnp.concatenate([o_head[n * seqs:(n + 1) * seqs] for n in range(heads)], axis=1)
    for piece in small_copies[1:]:
        piece.wait()
    wo_copy.wait()
    out[...] = jnp.dot(att, wo[...], preferred_element_type=jnp.float32).astype(out.dtype)


def attention(residual, gain, w_query, w_out, bias, lengths, keys, values, small):
    seqs, width = residual.shape
    heads = bias.shape[0]
    cache, size = keys.shape[1:]
    hbm = pl.BlockSpec(memory_space=pltpu.HBM)
    vmem = pl.BlockSpec(memory_space=pltpu.VMEM)
    outs = [((seqs, w_out.shape[1]), jnp.bfloat16)] + [(one.shape, one.dtype) for one in small]
    small = [pltpu.with_memory_space_constraint(one, pltpu.HBM) for one in small]
    lengths = pltpu.with_memory_space_constraint(lengths, pltpu.HBM)
    bias = pltpu.with_memory_space_constraint(bias, pltpu.HBM)
    gain = pltpu.with_memory_space_constraint(gain.reshape(1, width), pltpu.HBM)
    return pl.pallas_call(
        attn_kernel,
        out_shape=[pltpu.VMEM(shape, dtype) for shape, dtype in outs],
        in_specs=[hbm] * (7 + len(small)),
        out_specs=[vmem] * len(outs),
        scratch_shapes=[
            pltpu.SMEM(lengths.shape, jnp.int32),
            pltpu.SMEM(bias.shape, jnp.float32),
            pltpu.VMEM((1, width), jnp.float32),
            pltpu.VMEM(w_query.shape, jnp.bfloat16),
            pltpu.VMEM(keys.shape, jnp.bfloat16),
            pltpu.VMEM(values.shape, jnp.bfloat16),
            pltpu.VMEM(w_out.shape, jnp.bfloat16),
            pltpu.VMEM((seqs * heads, size), jnp.float32),
            pltpu.VMEM((seqs * heads, cache), jnp.float32),
            pltpu.VMEM((seqs * heads, size), jnp.float32),
            pltpu.SemaphoreType.DMA(()),
            pltpu.SemaphoreType.DMA(()),
            pltpu.SemaphoreType.DMA((COPIES,)),
            pltpu.SemaphoreType.DMA((COPIES,)),
            pltpu.SemaphoreType.DMA((len(small),)),
            pltpu.SemaphoreType.DMA(()),
            pltpu.SemaphoreType.DMA(()),
            pltpu.SemaphoreType.DMA(()),
        ],
        name="attend",
    )(lengths, bias, gain, w_query, keys, values, w_out, *small)


def call(kernel, outs, args, flops=0, vmem=16):
    in_vmem = pl.BlockSpec(memory_space=pltpu.VMEM)
    in_smem = pl.BlockSpec(memory_space=pltpu.SMEM)
    return pl.pallas_call(
        kernel,
        out_shape=[pltpu.VMEM(shape, dtype) for shape, dtype in outs],
        in_specs=[in_smem if arg.ndim == 1 else in_vmem for arg in args],
        out_specs=[in_vmem] * len(outs),
        compiler_params=pltpu.CompilerParams(vmem_limit_bytes=vmem << 20),
        cost_estimate=pl.CostEstimate(flops=flops, transcendentals=0, bytes_accessed=0),
    )(*args)


def route_kernel(count, *refs):
    parts = refs[:count]
    residual, gain, group_w, expert_w, routes, outgoing, mid_own, placing = refs[count:]
    total = sum(part[...].astype(jnp.float32) for part in parts)
    mid = residual[...].astype(jnp.float32) + total.astype(jnp.bfloat16).astype(jnp.float32)
    mid = mid.astype(jnp.bfloat16)
    values = mid.astype(jnp.float32)
    seqs, width = values.shape
    inverse = lax.rsqrt(jnp.mean(values * values, axis=-1, keepdims=True) + EPSILON)
    hidden = (values * inverse * gain[...]).astype(jnp.bfloat16)

    def logits(weight):
        return lax.dot_general(
            hidden, weight[...], (((1,), (1,)), ((), ())), preferred_element_type=jnp.float32
        )

    group_logit = logits(group_w)
    expert_logit = logits(expert_w)
    eye = lax.broadcasted_iota(jnp.int32, (TOPK, TOPK), 0)
    eye = (eye == lax.broadcasted_iota(jnp.int32, (TOPK, TOPK), 1)).astype(jnp.bfloat16)
    turned = lax.dot_general(
        routes[...].astype(jnp.float32).astype(jnp.bfloat16),
        eye,
        (((0,), (0,)), ((), ())),
        preferred_element_type=jnp.float32,
    ).astype(jnp.int32)
    named = [turned[:, k : k + 1] for k in range(TOPK)]
    group = jnp.right_shift(named[0], 3)
    member = [jnp.bitwise_and(one, GROUP_SIZE - 1) for one in named]
    lane_e = lax.broadcasted_iota(jnp.int32, expert_logit.shape, 1)
    lane_g = lax.broadcasted_iota(jnp.int32, group_logit.shape, 1)
    picked = [
        jnp.sum(jnp.where(lane_e == one, expert_logit, 0.0), axis=1, keepdims=True)
        for one in named
    ]
    most = functools.reduce(jnp.maximum, picked)
    powers = [jnp.exp(one - most) for one in picked]
    group_power = jnp.exp(group_logit - jnp.max(group_logit, axis=1, keepdims=True))
    in_group = lane_g == group
    top = jnp.sum(jnp.where(in_group, group_power, 0.0), axis=1, keepdims=True)
    top = top / jnp.sum(group_power, axis=1, keepdims=True)
    scale = top / sum(powers)
    lane = lax.broadcasted_iota(jnp.int32, (seqs, EXTRA), 1)
    half = EXTRA // 2
    spread = jnp.zeros((seqs, EXTRA), jnp.float32)
    for one, power in zip(member, powers):
        spread = jnp.where(jnp.bitwise_and(lane, half - 1) == one, power * scale, spread)
    high = spread.astype(jnp.bfloat16).astype(jnp.float32)
    extra = jnp.where(lane < half, high, spread - high).astype(jnp.bfloat16)
    before = lax.broadcasted_iota(jnp.int32, (seqs, seqs), 0)
    before = before > lax.broadcasted_iota(jnp.int32, (seqs, seqs), 1)
    hot = in_group.astype(jnp.float32)
    earlier = jnp.dot(
        before.astype(jnp.bfloat16), hot.astype(jnp.bfloat16), preferred_element_type=jnp.float32
    )
    rank = jnp.sum(earlier * hot, axis=1, keepdims=True).astype(jnp.int32)
    slot = group * GROUP_SIZE + rank
    slots = outgoing.shape[0]
    puts = (lax.broadcasted_iota(jnp.int32, (seqs, slots), 1) == slot).astype(jnp.bfloat16)
    placing[...] = puts

    def placed(value):
        out = lax.dot_general(
            puts, value, (((0,), (0,)), ((), ())), preferred_element_type=jnp.float32
        )
        return out.astype(jnp.bfloat16)

    outgoing[:, :width] = placed(hidden)
    outgoing[:, width:] = placed(extra)
    own = mid_own.shape[1]
    low = lax.broadcasted_iota(jnp.int32, (1, 1), 0) + lax.axis_index("tp")
    kept = jnp.zeros(mid_own.shape, jnp.float32)
    for n in range(width // own):
        kept = jnp.where(low == n, values[:, n * own : (n + 1) * own], kept)
    mid_own[...] = kept.astype(jnp.bfloat16)


def fetch_kernel(after, *refs):
    count = (len(refs) - 1) // 2
    sem = refs[-1]
    copies = [
        pltpu.make_async_copy(src, dst, sem.at[n])
        for n, (src, dst) in enumerate(zip(refs[:count], refs[count : 2 * count]))
    ]
    for piece in copies:
        piece.start()
    for piece in copies:
        piece.wait()


def fetched(arrays, after):
    hbm = pl.BlockSpec(memory_space=pltpu.HBM)
    vmem = pl.BlockSpec(memory_space=pltpu.VMEM)
    arrays = [pltpu.with_memory_space_constraint(one, pltpu.HBM) for one in arrays]
    return pl.pallas_call(
        fetch_kernel,
        out_shape=[pltpu.VMEM(one.shape, one.dtype) for one in arrays],
        in_specs=[vmem] + [hbm] * len(arrays),
        out_specs=[vmem] * len(arrays),
        scratch_shapes=[pltpu.SemaphoreType.DMA((len(arrays),))],
        compiler_params=pltpu.CompilerParams(vmem_limit_bytes=4 << 20),
        cost_estimate=pl.CostEstimate(flops=1 << 30, transcendentals=0, bytes_accessed=0),
        name="fetch",
    )(after, *arrays)


def expert_kernel(count, *refs):
    pieces = refs[:count]
    gate_w, up_w, down_w, kept, sent = refs[count:]
    width = gate_w.shape[0]
    rows = jnp.concatenate([piece[:, :width] for piece in pieces], axis=0)
    extra = jnp.concatenate([piece[:, width:] for piece in pieces], axis=0).astype(jnp.float32)
    lane = lax.broadcasted_iota(jnp.int32, extra.shape, 1)
    mine = jnp.bitwise_and(lane, EXTRA // 2 - 1) == lax.rem(lax.axis_index("ep"), GROUP_SIZE)
    weight = jnp.sum(jnp.where(mine, extra, 0.0), axis=1, keepdims=True)
    gate = jnp.dot(rows, gate_w[...], preferred_element_type=jnp.float32)
    upward = jnp.dot(rows, up_w[...], preferred_element_type=jnp.float32)
    active = (gate / (1.0 + jnp.exp(-gate)) * upward).astype(jnp.bfloat16)
    part = jnp.dot(active, down_w[...], preferred_element_type=jnp.float32) * weight
    own = kept.shape[0]
    kept[...] = part[:own].astype(jnp.bfloat16)
    sent[...] = part[own:].astype(jnp.bfloat16)


def experts(ours, theirs, weights):
    width = weights[2].shape[1]
    rows = sum(piece.shape[0] for piece in ours)
    out = ((rows, width), jnp.bfloat16)
    count = len(ours) + len(theirs)
    flops = 2 * 2 * rows * 3 * width * weights[0].shape[1]
    kernel = functools.partial(expert_kernel, count)
    return call(kernel, [out, out], [*ours, *theirs, *weights], flops)


def add_kernel(kept, arrived, *outs):
    rows = outs[0].shape[0]
    for n, out in enumerate(outs):
        part = slice(n * rows, (n + 1) * rows)
        total = kept[part].astype(jnp.float32) + arrived[part].astype(jnp.float32)
        out[...] = total.astype(jnp.bfloat16)


def block_kernel(count, *refs):
    parts, outs = refs[:count], refs[count:]
    steps, block = len(outs), outs[0].shape[1]
    for step in range(steps):
        start = pl.multiple_of(lax.rem(lax.axis_index("tp") + step, steps) * block, block)
        part = pl.ds(start, block)
        total = sum(one[:, part].astype(jnp.float32) for one in parts)
        outs[step][...] = total.astype(jnp.bfloat16)


def sum_kernel(*refs):
    refs[-1][...] = sum(one[...].astype(jnp.float32) for one in refs[:-1]).astype(jnp.bfloat16)


def last_kernel(mid_own, placing, returned, out):
    moe = jnp.dot(placing[...], returned[...], preferred_element_type=jnp.float32)
    out[...] = (mid_own[...].astype(jnp.float32) + moe).astype(jnp.bfloat16)


def per_device(
    residual,
    routes,
    lengths,
    key_cache,
    value_cache,
    mix_gain,
    w_query,
    w_out,
    head_bias,
    moe_gain,
    w_group,
    w_expert,
    expert_gate,
    expert_up,
    expert_down,
):
    bf16 = jnp.bfloat16
    seq_count, width = residual.shape
    n_tp = lax.axis_size("tp")
    own_width = width // n_tp
    slots = w_group.shape[1] * GROUP_SIZE

    head_part, *small = attention(
        residual,
        mix_gain,
        w_query,
        w_out,
        head_bias,
        lengths,
        key_cache.reshape(key_cache.shape[0], key_cache.shape[1], key_cache.shape[3]),
        value_cache.reshape(value_cache.shape[0], value_cache.shape[1], value_cache.shape[3]),
        [residual, moe_gain.reshape(1, width), w_group.T, w_expert.T],
    )
    weights = fetched((expert_gate[0], expert_up[0], expert_down[0]), head_part)
    head_parts = [head_part]
    for step in (1, 3, 2):
        part = tp_shift(head_part, step)
        head_parts.append(pltpu.with_memory_space_constraint(part, pltpu.VMEM))
    outgoing, mid_own, placing = call(
        functools.partial(route_kernel, n_tp),
        [
            ((slots, width + EXTRA), bf16),
            ((seq_count, own_width), bf16),
            ((seq_count, slots), bf16),
        ],
        [
            *head_parts,
            *small,
            routes.T,
        ],
    )
    arrived = z_exchange(outgoing.reshape(NZ, GROUP_SIZE, width + EXTRA))
    arrived = arrived.reshape(slots, width + EXTRA)

    def chunk(pieces):
        theirs = []
        for piece in pieces:
            theirs.append(core_swap(piece))
        kept, sent = experts(pieces, theirs, weights)
        return kept, core_swap(sent)

    def added(pair, count):
        rows = pair[0].shape[0] // count
        return call(add_kernel, [((rows, width), bf16)] * count, list(pair), vmem=8)

    half = slots // 2
    left = x_shift(arrived, 1)
    right = x_shift(arrived, -1)
    near = chunk([arrived])
    relay0 = x_shift(left[:half], 1)
    relay1 = x_shift(right[half:], -1)
    to_left, to_right = added(chunk([left, right]), 2)
    back0 = x_shift(to_left, -1)
    back1 = x_shift(to_right, 1)
    far = chunk([relay0, relay1])

    def y_sum(parts):
        blocks = call(
            functools.partial(block_kernel, len(parts)),
            [((slots, own_width), bf16)] * n_tp,
            list(parts),
            vmem=8,
        )
        summed = [blocks[0]]
        for step in (1, 3, 2):
            summed.append(tp_shift(blocks[step], step))
        return summed

    def total(parts):
        return call(sum_kernel, [((slots, own_width), bf16)], parts, vmem=4)[0]

    to_far = total(y_sum(far))
    own = y_sum([*near, back0, back1])
    back2 = x_shift(to_far, 2)
    total = total([*own, back2])
    returned = z_exchange(total.reshape(NZ, GROUP_SIZE, own_width)).reshape(slots, own_width)
    vmem = pl.BlockSpec(memory_space=pltpu.VMEM)
    return pl.pallas_call(
        last_kernel,
        out_shape=jax.ShapeDtypeStruct((seq_count, own_width), bf16),
        in_specs=[vmem] * 3,
        out_specs=vmem,
        compiler_params=pltpu.CompilerParams(vmem_limit_bytes=4 << 20),
        name="last",
    )(mid_own, placing, returned)


def solution(mesh):
    in_specs = (
        P("ep", None),
        P("ep", None),
        P("ep"),
        P("ep", None, "tp", None),
        P("ep", None, "tp", None),
        P(),
        P(None, "tp"),
        P("tp", None),
        P("tp"),
        P(),
        P(),
        P(),
        P("ep", None, "tp"),
        P("ep", None, "tp"),
        P("ep", "tp", None),
    )
    out_specs = P("ep", "tp")
    return jax.shard_map(
        per_device, mesh=mesh, in_specs=in_specs, out_specs=out_specs, check_vma=False
    )
```

```python
import functools

import jax
import jax.numpy as jnp
from jax import lax
from jax.experimental import pallas as pl
from jax.experimental.pallas import tpu as pltpu
from jax.sharding import PartitionSpec as P


GROUP_SIZE = 8
TOPK = 4
NZ = 8
NX = 4
NC = 2
EXTRA = 128
COPIES = 1


EPSILON = 1e-06


def ep_index(z, x, c):
    return (z % NZ) * (NX * NC) + (x % NX) * NC + c % NC


def x_shift(value, step):
    perm = [
        (ep_index(z, x, c), ep_index(z, x + step, c))
        for z in range(NZ)
        for x in range(NX)
        for c in range(NC)
    ]
    return lax.ppermute(value, "ep", perm)


def core_swap(value):
    perm = [(i, i ^ 1) for i in range(NZ * NX * NC)]
    return lax.ppermute(value, "ep", perm)


def tp_shift(value, step):
    n = lax.axis_size("tp")
    return lax.ppermute(value, "tp", [(i, (i + step) % n) for i in range(n)])


def z_exchange(value):
    groups = [[z * NX * NC + r for z in range(NZ)] for r in range(NX * NC)]
    return lax.all_to_all(
        value, "ep", split_axis=0, concat_axis=0, axis_index_groups=groups, tiled=True
    )


def split_in_kernel(value, parts):
    out = []
    for _ in range(parts):
        part = value.astype(jnp.bfloat16)
        out.append(part)
        value = value - part.astype(jnp.float32)
    return out


def attn_kernel(lengths_hbm, bias_hbm, gain_hbm, wq_hbm, k_hbm, v_hbm, wo_hbm, *refs):
    small = refs[:1]
    out, smalls = refs[1], refs[2:3]
    residual = smalls[0]
    (lengths, bias, gain, wq, k, v, wo, q_rows, s_rows, o_rows, wq_sem, wo_sem, k_sem, v_sem, small_sem,
     gain_sem, lengths_sem, bias_sem) = refs[3:]
    seqs, _ = residual.shape
    cache = k.shape[1]
    heads = q_rows.shape[0] // seqs
    size = k.shape[2]
    rows = seqs * heads
    groups = k_sem.shape[0]
    each = seqs // groups
    wq_copy = pltpu.make_async_copy(wq_hbm, wq, wq_sem)
    wo_copy = pltpu.make_async_copy(wo_hbm, wo, wo_sem)

    def copy(src, dst, sem, n):
        part = pl.ds(n * each, each)
        return pltpu.make_async_copy(src.at[part], dst.at[part], sem.at[n])

    k_copies = [copy(k_hbm, k, k_sem, n) for n in range(groups)]
    v_copies = [copy(v_hbm, v, v_sem, n) for n in range(groups)]
    small_copies = [
        pltpu.make_async_copy(src, dst, small_sem.at[n])
        for n, (src, dst) in enumerate(zip(small, smalls))
    ]
    gain_copy = pltpu.make_async_copy(gain_hbm, gain, gain_sem)
    lengths_copy = pltpu.make_async_copy(lengths_hbm, lengths, lengths_sem)
    bias_copy = pltpu.make_async_copy(bias_hbm, bias, bias_sem)
    lengths_copy.start()
    bias_copy.start()
    first = [gain_copy, small_copies[0], wq_copy, *k_copies, *v_copies[:-1]]
    for piece in [*first, wo_copy, v_copies[-1], *small_copies[1:]]:
        piece.start()
    gain_copy.wait()
    small_copies[0].wait()
    x = residual[...].astype(jnp.float32)
    inverse = lax.rsqrt(jnp.mean(x * x, axis=-1, keepdims=True) + EPSILON)
    normed = (x * inverse * gain[...]).astype(jnp.bfloat16)
    r = lax.broadcasted_iota(jnp.int32, (rows, rows), 0)
    c = lax.broadcasted_iota(jnp.int32, (rows, rows), 1)
    perm = (c == (r % heads) * seqs + r // heads).astype(jnp.bfloat16)
    row = lax.broadcasted_iota(jnp.int32, (rows, 1), 0)
    lengths_copy.wait()
    bias_copy.wait()
    b = jnp.zeros((rows, 1), jnp.float32)
    for n in range(heads):
        b = jnp.where(row % heads == n, bias[n], b)
    length = jnp.zeros((rows, 1), jnp.int32)
    for t in range(seqs):
        length = jnp.where(row // heads == t, lengths[t], length)
    inside = lax.broadcasted_iota(jnp.int32, (rows, cache), 1) < length
    wq_copy.wait()
    q = jnp.dot(normed, wq[...], preferred_element_type=jnp.float32).astype(jnp.bfloat16)
    q_head = jnp.concatenate([q[:, g * size:(g + 1) * size] for g in range(heads)], axis=0)
    q_rows[...] = jnp.dot(perm, q_head, preferred_element_type=jnp.float32)

    per = 8 // heads
    low = lax.broadcasted_iota(jnp.int32, (8, cache), 0) // heads
    low_o = lax.broadcasted_iota(jnp.int32, (8, size), 0) // heads
    for n in range(groups):
        k_copies[n].wait()
        for i in range(n * each // per, (n + 1) * each // per):
            q8 = q_rows[i * 8:(i + 1) * 8, :].astype(jnp.bfloat16)
            total = None
            for u in range(per):
                s = lax.dot_general(q8, k[i * per + u], (((1,), (1,)), ((), ())),
                                    preferred_element_type=jnp.float32)
                total = s if total is None else jnp.where(low == u, s, total)
            s_rows[i * 8:(i + 1) * 8, :] = total

    z = s_rows[...] * size ** (-0.5) + b
    remain = jnp.where(inside, -(jnp.maximum(z, 0.0) + jnp.log1p(jnp.exp(-jnp.abs(z)))), 0.0)
    first = lax.broadcasted_iota(jnp.int32, (cache, cache), 0)
    second = lax.broadcasted_iota(jnp.int32, (cache, cache), 1)
    later = (first >= second).astype(jnp.bfloat16)
    total = sum(
        jnp.dot(p, later, preferred_element_type=jnp.float32) for p in split_in_kernel(remain, 3)
    )
    s_rows[...] = jnp.where(inside, jnp.exp(z + total), 0.0)

    for n in range(groups):
        v_copies[n].wait()
        for i in range(n * each // per, (n + 1) * each // per):
            w8 = s_rows[i * 8:(i + 1) * 8, :].astype(jnp.bfloat16)
            total = None
            for u in range(per):
                o = jnp.dot(w8, v[i * per + u], preferred_element_type=jnp.float32)
                total = o if total is None else jnp.where(low_o == u, o, total)
            o_rows[i * 8:(i + 1) * 8, :] = total

    o_head = lax.dot_general(perm, o_rows[...].astype(jnp.bfloat16), (((0,), (0,)), ((), ())),
                             preferred_element_type=jnp.float32).astype(jnp.bfloat16)
    att = jnp.concatenate([o_head[n * seqs:(n + 1) * seqs] for n in range(heads)], axis=1)
    for piece in small_copies[1:]:
        piece.wait()
    wo_copy.wait()
    out[...] = jnp.dot(att, wo[...], preferred_element_type=jnp.float32).astype(out.dtype)


def attention(residual, gain, w_query, w_out, bias, lengths, keys, values, small):
    seqs, width = residual.shape
    heads = bias.shape[0]
    cache, size = keys.shape[1:]
    hbm = pl.BlockSpec(memory_space=pltpu.HBM)
    vmem = pl.BlockSpec(memory_space=pltpu.VMEM)
    outs = [((seqs, w_out.shape[1]), jnp.bfloat16)] + [(one.shape, one.dtype) for one in small]
    small = [pltpu.with_memory_space_constraint(one, pltpu.HBM) for one in small]
    lengths = pltpu.with_memory_space_constraint(lengths, pltpu.HBM)
    bias = pltpu.with_memory_space_constraint(bias, pltpu.HBM)
    gain = pltpu.with_memory_space_constraint(gain.reshape(1, width), pltpu.HBM)
    return pl.pallas_call(
        attn_kernel,
        out_shape=[pltpu.VMEM(shape, dtype) for shape, dtype in outs],
        in_specs=[hbm] * (7 + len(small)),
        out_specs=[vmem] * len(outs),
        scratch_shapes=[
            pltpu.SMEM(lengths.shape, jnp.int32),
            pltpu.SMEM(bias.shape, jnp.float32),
            pltpu.VMEM((1, width), jnp.float32),
            pltpu.VMEM(w_query.shape, jnp.bfloat16),
            pltpu.VMEM(keys.shape, jnp.bfloat16),
            pltpu.VMEM(values.shape, jnp.bfloat16),
            pltpu.VMEM(w_out.shape, jnp.bfloat16),
            pltpu.VMEM((seqs * heads, size), jnp.float32),
            pltpu.VMEM((seqs * heads, cache), jnp.float32),
            pltpu.VMEM((seqs * heads, size), jnp.float32),
            pltpu.SemaphoreType.DMA(()),
            pltpu.SemaphoreType.DMA(()),
            pltpu.SemaphoreType.DMA((COPIES,)),
            pltpu.SemaphoreType.DMA((COPIES,)),
            pltpu.SemaphoreType.DMA((len(small),)),
            pltpu.SemaphoreType.DMA(()),
            pltpu.SemaphoreType.DMA(()),
            pltpu.SemaphoreType.DMA(()),
        ],
        name="attend",
    )(lengths, bias, gain, w_query, keys, values, w_out, *small)


def call(kernel, outs, args, flops=0, vmem=16):
    in_vmem = pl.BlockSpec(memory_space=pltpu.VMEM)
    in_smem = pl.BlockSpec(memory_space=pltpu.SMEM)
    return pl.pallas_call(
        kernel,
        out_shape=[pltpu.VMEM(shape, dtype) for shape, dtype in outs],
        in_specs=[in_smem if arg.ndim == 1 else in_vmem for arg in args],
        out_specs=[in_vmem] * len(outs),
        compiler_params=pltpu.CompilerParams(vmem_limit_bytes=vmem << 20),
        cost_estimate=pl.CostEstimate(flops=flops, transcendentals=0, bytes_accessed=0),
    )(*args)


def route_kernel(count, *refs):
    parts = refs[:count]
    residual, gain, group_w, expert_w, routes, outgoing, mid_own, placing = refs[count:]
    total = sum(part[...].astype(jnp.float32) for part in parts)
    mid = residual[...].astype(jnp.float32) + total.astype(jnp.bfloat16).astype(jnp.float32)
    mid = mid.astype(jnp.bfloat16)
    values = mid.astype(jnp.float32)
    seqs, width = values.shape
    inverse = lax.rsqrt(jnp.mean(values * values, axis=-1, keepdims=True) + EPSILON)
    hidden = (values * inverse * gain[...]).astype(jnp.bfloat16)

    def logits(weight):
        return lax.dot_general(
            hidden, weight[...], (((1,), (1,)), ((), ())), preferred_element_type=jnp.float32
        )

    group_logit = logits(group_w)
    expert_logit = logits(expert_w)
    eye = lax.broadcasted_iota(jnp.int32, (TOPK, TOPK), 0)
    eye = (eye == lax.broadcasted_iota(jnp.int32, (TOPK, TOPK), 1)).astype(jnp.bfloat16)
    turned = lax.dot_general(
        routes[...].astype(jnp.float32).astype(jnp.bfloat16),
        eye,
        (((0,), (0,)), ((), ())),
        preferred_element_type=jnp.float32,
    ).astype(jnp.int32)
    named = [turned[:, k : k + 1] for k in range(TOPK)]
    group = jnp.right_shift(named[0], 3)
    member = [jnp.bitwise_and(one, GROUP_SIZE - 1) for one in named]
    lane_e = lax.broadcasted_iota(jnp.int32, expert_logit.shape, 1)
    lane_g = lax.broadcasted_iota(jnp.int32, group_logit.shape, 1)
    picked = [
        jnp.sum(jnp.where(lane_e == one, expert_logit, 0.0), axis=1, keepdims=True)
        for one in named
    ]
    most = functools.reduce(jnp.maximum, picked)
    powers = [jnp.exp(one - most) for one in picked]
    group_power = jnp.exp(group_logit - jnp.max(group_logit, axis=1, keepdims=True))
    in_group = lane_g == group
    top = jnp.sum(jnp.where(in_group, group_power, 0.0), axis=1, keepdims=True)
    top = top / jnp.sum(group_power, axis=1, keepdims=True)
    scale = top / sum(powers)
    lane = lax.broadcasted_iota(jnp.int32, (seqs, EXTRA), 1)
    half = EXTRA // 2
    spread = jnp.zeros((seqs, EXTRA), jnp.float32)
    for one, power in zip(member, powers):
        spread = jnp.where(jnp.bitwise_and(lane, half - 1) == one, power * scale, spread)
    high = spread.astype(jnp.bfloat16).astype(jnp.float32)
    extra = jnp.where(lane < half, high, spread - high).astype(jnp.bfloat16)
    before = lax.broadcasted_iota(jnp.int32, (seqs, seqs), 0)
    before = before > lax.broadcasted_iota(jnp.int32, (seqs, seqs), 1)
    hot = in_group.astype(jnp.float32)
    earlier = jnp.dot(
        before.astype(jnp.bfloat16), hot.astype(jnp.bfloat16), preferred_element_type=jnp.float32
    )
    rank = jnp.sum(earlier * hot, axis=1, keepdims=True).astype(jnp.int32)
    slot = group * GROUP_SIZE + rank
    slots = outgoing.shape[0]
    puts = (lax.broadcasted_iota(jnp.int32, (seqs, slots), 1) == slot).astype(jnp.bfloat16)
    placing[...] = puts

    def placed(value):
        out = lax.dot_general(
            puts, value, (((0,), (0,)), ((), ())), preferred_element_type=jnp.float32
        )
        return out.astype(jnp.bfloat16)

    outgoing[:, :width] = placed(hidden)
    outgoing[:, width:] = placed(extra)
    own = mid_own.shape[1]
    low = lax.broadcasted_iota(jnp.int32, (1, 1), 0) + lax.axis_index("tp")
    kept = jnp.zeros(mid_own.shape, jnp.float32)
    for n in range(width // own):
        kept = jnp.where(low == n, values[:, n * own : (n + 1) * own], kept)
    mid_own[...] = kept.astype(jnp.bfloat16)


def fetch_kernel(after, *refs):
    count = (len(refs) - 1) // 2
    sem = refs[-1]
    copies = [
        pltpu.make_async_copy(src, dst, sem.at[n])
        for n, (src, dst) in enumerate(zip(refs[:count], refs[count : 2 * count]))
    ]
    for piece in copies:
        piece.start()
    for piece in copies:
        piece.wait()


def fetched(arrays, after):
    hbm = pl.BlockSpec(memory_space=pltpu.HBM)
    vmem = pl.BlockSpec(memory_space=pltpu.VMEM)
    arrays = [pltpu.with_memory_space_constraint(one, pltpu.HBM) for one in arrays]
    return pl.pallas_call(
        fetch_kernel,
        out_shape=[pltpu.VMEM(one.shape, one.dtype) for one in arrays],
        in_specs=[vmem] + [hbm] * len(arrays),
        out_specs=[vmem] * len(arrays),
        scratch_shapes=[pltpu.SemaphoreType.DMA((len(arrays),))],
        compiler_params=pltpu.CompilerParams(vmem_limit_bytes=4 << 20),
        cost_estimate=pl.CostEstimate(flops=1 << 30, transcendentals=0, bytes_accessed=0),
        name="fetch",
    )(after, *arrays)


def expert_kernel(count, *refs):
    pieces = refs[:count]
    gate_w, up_w, down_w, kept, sent = refs[count:]
    width = gate_w.shape[0]
    rows = jnp.concatenate([piece[:, :width] for piece in pieces], axis=0)
    extra = jnp.concatenate([piece[:, width:] for piece in pieces], axis=0).astype(jnp.float32)
    lane = lax.broadcasted_iota(jnp.int32, extra.shape, 1)
    mine = jnp.bitwise_and(lane, EXTRA // 2 - 1) == lax.rem(lax.axis_index("ep"), GROUP_SIZE)
    weight = jnp.sum(jnp.where(mine, extra, 0.0), axis=1, keepdims=True)
    gate = jnp.dot(rows, gate_w[...], preferred_element_type=jnp.float32)
    upward = jnp.dot(rows, up_w[...], preferred_element_type=jnp.float32)
    active = (gate / (1.0 + jnp.exp(-gate)) * upward).astype(jnp.bfloat16)
    part = jnp.dot(active, down_w[...], preferred_element_type=jnp.float32) * weight
    own = kept.shape[0]
    kept[...] = part[:own].astype(jnp.bfloat16)
    sent[...] = part[own:].astype(jnp.bfloat16)


def experts(ours, theirs, weights):
    width = weights[2].shape[1]
    rows = sum(piece.shape[0] for piece in ours)
    out = ((rows, width), jnp.bfloat16)
    count = len(ours) + len(theirs)
    flops = 2 * 2 * rows * 3 * width * weights[0].shape[1]
    kernel = functools.partial(expert_kernel, count)
    return call(kernel, [out, out], [*ours, *theirs, *weights], flops)


def add_kernel(kept, arrived, *outs):
    rows = outs[0].shape[0]
    for n, out in enumerate(outs):
        part = slice(n * rows, (n + 1) * rows)
        total = kept[part].astype(jnp.float32) + arrived[part].astype(jnp.float32)
        out[...] = total.astype(jnp.bfloat16)


def block_kernel(count, *refs):
    parts, outs = refs[:count], refs[count:]
    steps, block = len(outs), outs[0].shape[1]
    for step in range(steps):
        start = pl.multiple_of(lax.rem(lax.axis_index("tp") + step, steps) * block, block)
        part = pl.ds(start, block)
        total = sum(one[:, part].astype(jnp.float32) for one in parts)
        outs[step][...] = total.astype(jnp.bfloat16)


def sum_kernel(*refs):
    refs[-1][...] = sum(one[...].astype(jnp.float32) for one in refs[:-1]).astype(jnp.bfloat16)


def last_kernel(mid_own, placing, returned, out):
    moe = jnp.dot(placing[...], returned[...], preferred_element_type=jnp.float32)
    out[...] = (mid_own[...].astype(jnp.float32) + moe).astype(jnp.bfloat16)


def per_device(
    residual,
    routes,
    lengths,
    key_cache,
    value_cache,
    mix_gain,
    w_query,
    w_out,
    head_bias,
    moe_gain,
    w_group,
    w_expert,
    expert_gate,
    expert_up,
    expert_down,
):
    bf16 = jnp.bfloat16
    seq_count, width = residual.shape
    n_tp = lax.axis_size("tp")
    own_width = width // n_tp
    slots = w_group.shape[1] * GROUP_SIZE

    head_part, *small = attention(
        residual,
        mix_gain,
        w_query,
        w_out,
        head_bias,
        lengths,
        key_cache.reshape(key_cache.shape[0], key_cache.shape[1], key_cache.shape[3]),
        value_cache.reshape(value_cache.shape[0], value_cache.shape[1], value_cache.shape[3]),
        [residual],
    )
    tables = (moe_gain.reshape(1, width), w_group.T, w_expert.T)
    weights = (expert_gate[0], expert_up[0], expert_down[0])
    fetch = fetched((*tables, *weights), head_part)
    tables, weights = fetch[:3], fetch[3:]
    head_parts = [head_part]
    for step in (1, 3, 2):
        part = tp_shift(head_part, step)
        head_parts.append(pltpu.with_memory_space_constraint(part, pltpu.VMEM))
    outgoing, mid_own, placing = call(
        functools.partial(route_kernel, n_tp),
        [
            ((slots, width + EXTRA), bf16),
            ((seq_count, own_width), bf16),
            ((seq_count, slots), bf16),
        ],
        [
            *head_parts,
            *small,
            *tables,
            routes.T,
        ],
    )
    arrived = z_exchange(outgoing.reshape(NZ, GROUP_SIZE, width + EXTRA))
    arrived = arrived.reshape(slots, width + EXTRA)

    def chunk(pieces):
        theirs = []
        for piece in pieces:
            theirs.append(core_swap(piece))
        kept, sent = experts(pieces, theirs, weights)
        return kept, core_swap(sent)

    def added(pair, count):
        rows = pair[0].shape[0] // count
        return call(add_kernel, [((rows, width), bf16)] * count, list(pair), vmem=8)

    half = slots // 2
    left = x_shift(arrived, 1)
    right = x_shift(arrived, -1)
    near = chunk([arrived])
    relay0 = x_shift(left[:half], 1)
    relay1 = x_shift(right[half:], -1)
    to_left, to_right = added(chunk([left, right]), 2)
    back0 = x_shift(to_left, -1)
    back1 = x_shift(to_right, 1)
    far = chunk([relay0, relay1])

    def y_sum(parts):
        blocks = call(
            functools.partial(block_kernel, len(parts)),
            [((slots, own_width), bf16)] * n_tp,
            list(parts),
            vmem=8,
        )
        summed = [blocks[0]]
        for step in (1, 3, 2):
            summed.append(tp_shift(blocks[step], step))
        return summed

    def total(parts):
        return call(sum_kernel, [((slots, own_width), bf16)], parts, vmem=4)[0]

    to_far = total(y_sum(far))
    own = y_sum([*near, back0, back1])
    back2 = x_shift(to_far, 2)
    total = total([*own, back2])
    returned = z_exchange(total.reshape(NZ, GROUP_SIZE, own_width)).reshape(slots, own_width)
    vmem = pl.BlockSpec(memory_space=pltpu.VMEM)
    return pl.pallas_call(
        last_kernel,
        out_shape=jax.ShapeDtypeStruct((seq_count, own_width), bf16),
        in_specs=[vmem] * 3,
        out_specs=vmem,
        compiler_params=pltpu.CompilerParams(vmem_limit_bytes=4 << 20),
        name="last",
    )(mid_own, placing, returned)


def solution(mesh):
    in_specs = (
        P("ep", None),
        P("ep", None),
        P("ep"),
        P("ep", None, "tp", None),
        P("ep", None, "tp", None),
        P(),
        P(None, "tp"),
        P("tp", None),
        P("tp"),
        P(),
        P(),
        P(),
        P("ep", None, "tp"),
        P("ep", None, "tp"),
        P("ep", "tp", None),
    )
    out_specs = P("ep", "tp")
    return jax.shard_map(
        per_device, mesh=mesh, in_specs=in_specs, out_specs=out_specs, check_vma=False
    )
```
